32 devices in a mesh: sp: 8 (over z, core), tp: 4 (over y, x).
Axes of the slice: x: 2, y: 2, z: 4, core: 2. Of those that a mesh axis runs over, the one named last changes fastest.
Arguments:
- query_a: bfloat16 [1536, 2048], P('sp', 'tp'), may hold values from -6 to 6
- key_a: bfloat16 [1536, 2048], P('sp', 'tp'), may hold values from -6 to 6
- value_a: bfloat16 [1536, 2048], P('sp', 'tp'), may hold values from -6 to 6
- query_b: bfloat16 [1536, 2048], P('sp', 'tp'), may hold values from -6 to 6
- key_b: bfloat16 [1536, 2048], P('sp', 'tp'), may hold values from -6 to 6
- value_b: bfloat16 [1536, 2048], P('sp', 'tp'), may hold values from -6 to 6
- stop_a: float32 [1536, 32], P('sp', 'tp'), may hold values from -14 to -1
- stop_b: float32 [1536, 16], P('sp', 'tp'), may hold values from -14 to -1
- out_a: bfloat16 [2048, 2048], P('tp'), may hold values from -4 to 4
- out_b: bfloat16 [2048, 2048], P('tp'), may hold values from -4 to 4
- resid: bfloat16 [1536, 2048], P('sp', 'tp'), may hold values from -20 to 20
- mix_gain: float32 [2048], P('tp'), may hold values from 0.1 to 1.9
- ffn_gain: float32 [2048], P('tp'), may hold values from 0.1 to 1.9
- routes: int32 [1536, 2], P('sp'), may hold values from 0 to 31, all different within a row; in each aligned block of 192 rows (0 to 191, 192 to 383, ...) at most 18 rows name the same one
- gates: float32 [1536, 2], P('sp'), may hold values from 0.25 to 1.5
- exp_gate: bfloat16 [32, 2048, 512], P('sp', 'tp'), may hold values from -0.125 to 0.125
- exp_up: bfloat16 [32, 2048, 512], P('sp', 'tp'), may hold values from -0.125 to 0.125
- exp_down: bfloat16 [32, 512, 2048], P('sp', None, 'tp'), may hold values from -0.25 to 0.25
- sh_gate: bfloat16 [2048, 512], P('tp'), may hold values from -0.125 to 0.125
- sh_up: bfloat16 [2048, 512], P('tp'), may hold values from -0.125 to 0.125
- sh_down: bfloat16 [512, 2048], P(None, 'tp'), may hold values from -4 to 4
Outputs:
- result: bfloat16 [1536, 2048], P('sp', 'tp')
The draws below stay inside these ranges and needn't reach their ends.
Inputs may be any that keep to these rules, and one draw needn't show every extreme that they name: `routes`: each row names 2 different experts. Within the rows of one index of sp (aligned blocks of 192 rows) no expert is named by more than 18 rows, a bound that some block reaches.
All inputs are finite; a program needn't handle non-finite values.
Results may differ from the reference program's by a relative error of at most 0.02.
Values may be sent and summed in bfloat16 or wider, within the bound.
A program may use at most 64 MiB of HBM per device.

```python
import math
import jax
import jax.numpy as jnp
import numpy as np
from jax import lax

D = 2048
HA = 32
HEAD_A = 64
HB = 16
HEAD_B = 128
F = 512
FS = 512
TOP_K = 2
TOK = 192
TOKENS = 1536
EXPERTS = 32
CAP = 18
N_SP = 8
N_TP = 4


def column_scales(key, columns):
    width = max(1, columns // 32)
    count = (columns + width - 1) // width
    levels = jnp.exp(jax.random.uniform(key, (count,), jnp.float32, math.log(0.33), math.log(3.0)))
    return levels[jnp.arange(columns) // width]


def scaled_normal(key, rows, columns, spread, scale_key):
    values = jnp.clip(jax.random.normal(key, (rows, columns), jnp.float32), -5.0, 5.0) * spread
    return values * column_scales(scale_key, columns)[None, :]


def stop_offsets(key, heads):
    parts = jax.random.split(key, 5)
    chance = jax.random.uniform(parts[0], (heads,), jnp.float32)
    slow = chance < 0.5
    base = jnp.where(slow, -math.log(TOKENS) - 0.5, -4.0)
    base = base + jax.random.uniform(parts[1], (heads,), jnp.float32, -0.5, 0.5)
    phase = jax.random.uniform(parts[2], (heads,), jnp.float32, 0.0, 2.0 * math.pi)
    position = jnp.arange(TOKENS, dtype=jnp.float32) / TOKENS
    trend = 0.8 * jnp.sin(6.0 * math.pi * position[:, None] + phase[None, :])
    count = (TOKENS + 7) // 8
    jitter = jax.random.uniform(parts[3], (count, heads), jnp.float32, -0.8, 0.8)[jnp.arange(TOKENS) // 8]
    rough = jax.random.uniform(parts[4], (TOKENS, heads), jnp.float32, -0.3, 0.3)
    return base[None, :] + trend + jitter + rough


def draw_stop_a(key, part):
    return stop_offsets(jax.random.fold_in(key, 21), HA)


def draw_stop_b(key, part):
    return stop_offsets(jax.random.fold_in(key, 22), HB)


def draw_out_a(key, part):
    spread = (HA * HEAD_A + HB * HEAD_B) ** (-0.5)
    values = scaled_normal(jax.random.fold_in(key, 31), HA * HEAD_A, D, spread, jax.random.fold_in(key, 7))
    return values.astype(jnp.bfloat16)


def draw_out_b(key, part):
    spread = (HA * HEAD_A + HB * HEAD_B) ** (-0.5)
    values = scaled_normal(jax.random.fold_in(key, 32), HB * HEAD_B, D, spread, jax.random.fold_in(key, 7))
    return values.astype(jnp.bfloat16)


def draw_resid(key, part):
    values = scaled_normal(jax.random.fold_in(key, 41), TOKENS, D, 1.0, jax.random.fold_in(key, 5))
    return values.astype(jnp.bfloat16)


def draw_sh_down(key, part):
    values = scaled_normal(jax.random.fold_in(key, 51), FS, D, FS ** (-0.5), jax.random.fold_in(key, 9))
    return values.astype(jnp.bfloat16)


def block_scale(stream_key, shape, cuts, least, top_value):
    def one(dim, blocks):
        heights = jax.random.uniform(jax.random.fold_in(jax.random.fold_in(stream_key, 6), dim), (blocks,), jnp.float32, least / len(cuts), top_value / len(cuts))
        return jnp.repeat(jnp.exp(heights), shape[dim] // blocks).reshape((-1,) + (1,) * (len(shape) - dim - 1))

    factor_of = one(*cuts[0])
    for cut in cuts[1:]:
        factor_of = factor_of * one(*cut)
    return factor_of


def deal_out(rng, own, number, rows, number_of, top, reach, skew):
    order = jax.random.permutation(rng, number_of)
    packed, ordinary = load_shares(number_of, rows * top, reach, skew, True), load_shares(number_of, rows * top, reach, skew, False)
    places = jnp.arange(number_of)

    def named(tallies, turn):
        used = int((tallies > 0).sum())
        fixed = max(1, used // 4)
        moved = fixed + (places - fixed + turn * (used - fixed)) % max(1, number_of - fixed)
        return jnp.zeros((number_of,), jnp.int32).at[order[jnp.where(places < fixed, places, moved)]].set(jnp.asarray(tallies, jnp.int32))

    tallies = jnp.where(number % 4 == 0, named(packed, number // 4), named(ordinary, number - number // 4 - 1))
    mixed = jax.random.permutation(jax.random.fold_in(own, 3), number_of)
    source_of, sink = mixed[0:number_of // 2 * 2:2], mixed[1:number_of // 2 * 2:2]
    slack = jnp.minimum(tallies[source_of] - 1, reach - tallies[sink]) // 2
    slack = jnp.where((source_of == order[0]) | (sink == order[0]) | (tallies[sink] == 0), 0, jnp.maximum(slack, 0))
    moved = jax.random.randint(jax.random.fold_in(own, 4), (number_of // 2,), 0, 1 << 20) % (slack + 1)
    tallies = tallies.at[source_of].add(-moved).at[sink].add(moved)
    labels = jnp.searchsorted(jnp.cumsum(tallies), jnp.arange(rows * top), side="right").astype(jnp.int32)
    grid = labels.reshape(top, rows).T
    grid = grid[jax.random.permutation(jax.random.fold_in(own, 1), rows)]
    turn = jax.random.randint(jax.random.fold_in(own, 2), (rows, 1), 0, top)
    return jnp.take_along_axis(grid, (jnp.arange(top)[None, :] + turn) % top, axis=1)


def load_shares(number_of, total, reach, slope, full):
    weights = [(1 << 20) // math.isqrt(standing ** slope) + 1 for standing in range(1, number_of + 1)]
    largest = reach if full else min(reach, max(-(-total // number_of), total * weights[0] // sum(weights)))
    least = 1 if total - largest >= number_of - 1 else 0
    given, surplus = [largest] + [least] * (number_of - 1), total - largest - least * (number_of - 1)
    while surplus > 0:
        movable = [i for i in range(1, number_of) if given[i] < largest] or [i for i in range(1, number_of) if given[i] < reach]
        pool, budget = sum([weights[i] for i in movable]), surplus
        for i in movable:
            more = min(reach - given[i], max(1, budget * weights[i] // pool), surplus)
            given[i] = given[i] + more
            surplus = surplus - more
    return np.array(given)


def scatter_about(stream_key, extent, deviation, most, cuts=(), kind=jnp.bfloat16):
    array = deviation * jax.random.normal(stream_key, extent, jnp.float32)
    if cuts:
        array = array * block_scale(stream_key, extent, cuts, -0.22, 0.18)
    return jnp.clip(array, -most, most).astype(kind)


def setup_inputs(seed: int = 0) -> dict:
    seeds = jax.random.split(jax.random.key(seed), 22)
    query_a = scatter_about(seeds[0], (TOKENS, HA * HEAD_A), 1.0, 6.0, ((0, 8), (1, 4)))
    key_a = scatter_about(seeds[1], (TOKENS, HA * HEAD_A), 1.0, 6.0, ((0, 8), (1, 4)))
    value_a = scatter_about(seeds[2], (TOKENS, HA * HEAD_A), 1.0, 6.0, ((0, 8), (1, 4)))
    query_b = scatter_about(seeds[3], (TOKENS, HB * HEAD_B), 1.0, 6.0, ((0, 8), (1, 4)))
    key_b = scatter_about(seeds[4], (TOKENS, HB * HEAD_B), 1.0, 6.0, ((0, 8), (1, 4)))
    value_b = scatter_about(seeds[5], (TOKENS, HB * HEAD_B), 1.0, 6.0, ((0, 8), (1, 4)))
    stop_a = draw_stop_a(jax.random.fold_in(seeds[21], 71), 0)
    stop_b = draw_stop_b(jax.random.fold_in(seeds[21], 71), 0)
    out_a = draw_out_a(jax.random.fold_in(seeds[21], 71), 0)
    out_b = draw_out_b(jax.random.fold_in(seeds[21], 71), 0)
    resid = draw_resid(jax.random.fold_in(seeds[21], 71), 0)
    mix_gain = jnp.clip(1.0 + 0.18 * jax.random.normal(seeds[11], (D,), jnp.float32), 0.1, 1.9)
    ffn_gain = jnp.clip(1.0 + 0.18 * jax.random.normal(seeds[12], (D,), jnp.float32), 0.1, 1.9)
    routes_keys = jax.random.split(jax.random.fold_in(seeds[13], 1), TOKENS // TOK)
    routes_turns = jax.random.permutation(jax.random.fold_in(seeds[13], 3), TOKENS // TOK)
    routes = jax.vmap(lambda own, number: deal_out(jax.random.fold_in(seeds[13], 2), own, number, TOK, EXPERTS, TOP_K, CAP, 1))(routes_keys, routes_turns).reshape((TOKENS, TOP_K))
    gates = jnp.clip(0.25 + 1.25 * jax.random.uniform(seeds[14], (TOKENS, TOP_K), jnp.float32) ** block_scale(seeds[14], (TOKENS, TOP_K), ((0, 8),), -0.2, 0.2), 0.25, 1.5)
    exp_gate = scatter_about(seeds[15], (EXPERTS, D, F), D ** -0.5, 0.125, ((0, 8), (1, 4)))
    exp_up = scatter_about(seeds[16], (EXPERTS, D, F), D ** -0.5, 0.125, ((0, 8), (1, 4)))
    exp_down = scatter_about(seeds[17], (EXPERTS, F, D), F ** -0.5, 0.25, ((0, 8), (2, 4)))
    sh_gate = scatter_about(seeds[18], (D, FS), D ** -0.5, 0.125, ((0, 4),))
    sh_up = scatter_about(seeds[19], (D, FS), D ** -0.5, 0.125, ((0, 4),))
    sh_down = draw_sh_down(jax.random.fold_in(seeds[21], 71), 0)
    return {"query_a": query_a, "key_a": key_a, "value_a": value_a, "query_b": query_b, "key_b": key_b, "value_b": value_b, "stop_a": stop_a, "stop_b": stop_b, "out_a": out_a, "out_b": out_b, "resid": resid, "mix_gain": mix_gain, "ffn_gain": ffn_gain, "routes": routes, "gates": gates, "exp_gate": exp_gate, "exp_up": exp_up, "exp_down": exp_down, "sh_gate": sh_gate, "sh_up": sh_up, "sh_down": sh_down}


epsilon = 1e-06

def stick_group(query, keys, values, stop, heads):
    size = query.shape[1] // heads
    scale = size ** (-0.5)
    blocks = TOKENS // TOK
    query_blocks = query.reshape(blocks, TOK, heads, size).astype(jnp.float32)
    key_blocks = keys.reshape(blocks, TOK, heads, size).astype(jnp.float32)
    value_blocks = values.reshape(blocks, TOK, heads, size).astype(jnp.float32)
    stop_blocks = stop.reshape(blocks, TOK, heads).astype(jnp.float32)
    places = jnp.arange(TOK, dtype=jnp.int32)

    def one_query_block(number):
        query_here = query_blocks[number]
        stop_here = jnp.transpose(stop_blocks[number])[:, :, None]

        def visit(offset, state):
            source = number - offset

            def work(inner):
                output, carried = inner
                safe = jnp.maximum(source, 0)
                key_here = key_blocks[safe]
                value_here = value_blocks[safe]
                scores = jnp.einsum('qhd,khd->hqk', query_here, key_here, precision=lax.Precision.HIGHEST) * scale + stop_here
                causal = (source * TOK + places)[None, :] < (number * TOK + places)[:, None]
                failing = jnp.where(causal[None], jax.nn.log_sigmoid(-scores), 0.0)
                after = lax.cumsum(failing, axis=2, reverse=True) - failing + carried[:, :, None]
                weight = jnp.where(causal[None], jnp.exp(jax.nn.log_sigmoid(scores) + after), 0.0)
                weight = lax.optimization_barrier(weight.astype(jnp.bfloat16)).astype(jnp.float32)
                output = output + jnp.einsum('hqk,khe->qhe', weight, value_here, precision=lax.Precision.HIGHEST)
                return (output, carried + lax.optimization_barrier(jnp.sum(failing, axis=2)))
            return lax.cond(source >= 0, work, lambda inner: inner, state)
        start = (jnp.zeros((TOK, heads, size), jnp.float32), jnp.zeros((heads, TOK), jnp.float32))
        output, _ = lax.fori_loop(0, blocks, visit, start)
        return output
    gathered = lax.map(one_query_block, jnp.arange(blocks, dtype=jnp.int32))
    return gathered.reshape(TOKENS, heads * size).astype(jnp.bfloat16)

def grouped_product(rows, weight):
    count = rows.shape[0]
    width = weight.shape[1]
    part_rows = rows.reshape(count, N_TP, D // N_TP).astype(jnp.float32)
    part_weight = weight.reshape(N_TP, D // N_TP, width).astype(jnp.float32)
    partial_value = jnp.einsum('rgd,gdf->grf', part_rows, part_weight, precision=lax.Precision.HIGHEST)
    rounded = lax.optimization_barrier(partial_value.astype(jnp.bfloat16))
    return lax.optimization_barrier(jnp.sum(rounded.astype(jnp.float32), axis=0))

def row_scale(values):
    return lax.rsqrt(lax.optimization_barrier(jnp.mean(values * values, axis=1, keepdims=True)) + epsilon)

def reference(query_a, key_a, value_a, query_b, key_b, value_b, stop_a, stop_b, out_a, out_b, resid, mix_gain, ffn_gain, routes, gates, exp_gate, exp_up, exp_down, sh_gate, sh_up, sh_down):
    attended_a = stick_group(query_a, key_a, value_a, stop_a, HA)
    attended_b = stick_group(query_b, key_b, value_b, stop_b, HB)
    rows_a = HA * HEAD_A // N_TP
    rows_b = HB * HEAD_B // N_TP
    sets_a = jnp.transpose(attended_a.reshape(TOKENS, N_TP, rows_a), (1, 0, 2))
    sets_b = jnp.transpose(attended_b.reshape(TOKENS, N_TP, rows_b), (1, 0, 2))
    weights_a = out_a.reshape(N_TP, rows_a, D)
    weights_b = out_b.reshape(N_TP, rows_b, D)

    def add_set(total, pieces):
        left_a, right_a, left_b, right_b = pieces
        partial_value = jnp.dot(left_a, right_a, preferred_element_type=jnp.float32)
        partial_value = partial_value + jnp.dot(left_b, right_b, preferred_element_type=jnp.float32)
        return (total + lax.optimization_barrier(partial_value.astype(jnp.bfloat16)).astype(jnp.float32), None)
    mixed, _ = lax.scan(add_set, jnp.zeros((TOKENS, D), jnp.float32), (sets_a, weights_a, sets_b, weights_b))
    branch = mixed * row_scale(mixed) * mix_gain.astype(jnp.float32)[None, :]
    stream = lax.optimization_barrier((resid.astype(jnp.float32) + branch).astype(jnp.bfloat16))
    stream_f = stream.astype(jnp.float32)
    normed = (stream_f * row_scale(stream_f) * ffn_gain.astype(jnp.float32)[None, :]).astype(jnp.bfloat16)
    pairs = routes.reshape(N_SP, TOK * TOP_K).astype(jnp.int32)
    onehot = (pairs[:, :, None] == jnp.arange(EXPERTS, dtype=jnp.int32)[None, None, :]).astype(jnp.int32)
    earlier = jnp.cumsum(onehot, axis=1) - onehot
    ranks = lax.optimization_barrier(jnp.sum(earlier * onehot, axis=2))
    group = jnp.arange(N_SP, dtype=jnp.int32)[:, None]
    index = ((pairs * N_SP + group) * CAP + ranks).reshape(-1).astype(jnp.int32)
    source_rows = jnp.repeat(jnp.arange(TOKENS, dtype=jnp.int32), TOP_K)
    buffer = jnp.zeros((EXPERTS * N_SP * CAP, D), jnp.bfloat16).at[index].set(normed[source_rows])
    buffer = buffer.reshape(EXPERTS, N_SP * CAP, D)

    def one_expert(pieces):
        rows_here, gate_here, up_here, down_here = pieces
        gate_pre = grouped_product(rows_here, gate_here)
        up_pre = grouped_product(rows_here, up_here)
        hidden = (jax.nn.silu(gate_pre) * up_pre).astype(jnp.bfloat16)
        return jnp.dot(hidden, down_here, preferred_element_type=jnp.float32).astype(jnp.bfloat16)
    produced = lax.map(one_expert, (buffer, exp_gate, exp_up, exp_down)).reshape(EXPERTS * N_SP * CAP, D)
    picked = produced[index].reshape(TOKENS, TOP_K, D).astype(jnp.float32)
    routed = lax.optimization_barrier(jnp.sum(gates.astype(jnp.float32)[:, :, None] * picked, axis=1))
    shared_gate = grouped_product(normed, sh_gate)
    shared_up = grouped_product(normed, sh_up)
    shared_hidden = (jax.nn.silu(shared_gate) * shared_up).astype(jnp.bfloat16)
    shared_out = jnp.dot(shared_hidden, sh_down, preferred_element_type=jnp.float32)
    moe = routed + shared_out
    result = stream_f + moe
    return result.astype(jnp.bfloat16)
```

```python
import functools
import math

import jax
import jax.numpy as jnp
import numpy as np
from jax import lax
from jax.experimental import pallas as pl
from jax.experimental.pallas import tpu as pltpu
from jax.sharding import PartitionSpec as P

MESH = pl.DeviceIdType.MESH
LANES = 128
LOG2E = 1.4426950408889634
epsilon = 1e-06
VM = pl.BlockSpec(memory_space=pltpu.VMEM)


def greet(axis, peers):
    barrier = pltpu.get_barrier_semaphore()
    for peer in peers:
        pl.semaphore_signal(barrier, inc=1, device_id={axis: peer}, device_id_type=MESH)
    pl.semaphore_wait(barrier, len(peers))


def params(cid):
    return pltpu.CompilerParams(
        collective_id=cid, has_side_effects=True, vmem_limit_bytes=56 * 1024 * 1024
    )


def snake(r, j, m):
    return m * r + (j if m % 2 == 0 else r - 1 - j)


def stick_kernel(n, rows, groups, offsets, *refs):
    g_count = len(groups)
    count = 3 * g_count + 1
    ins, outs = refs[:count], refs[count : count + g_count]
    full = refs[count + g_count : 2 * count + g_count]
    made = refs[2 * count + g_count : 2 * count + 2 * g_count]
    send, recv, rsend, rrecv, own, bsend, brecv = refs[2 * count + 2 * g_count :]
    me = lax.axis_index("sp")
    nz = n // 2
    z, c = me // 2, lax.rem(me, 2)
    partner = z * 2 + 1 - c
    places = [lax.rem(z + d, nz) for d in range(nz)]
    greet("sp", [lax.rem(me + d, n) for d in range(1, n)])
    order = [count - 1] + list(range(count - 1))

    def piece(t, place):
        if t == count - 1:
            return ins[t]
        unit = (2 * place) // (n // groups[t // 3][0])
        return ins[t].at[:, pl.ds(pl.multiple_of(unit * LANES, LANES), LANES)]

    def spot(t, source):
        tall = ins[t].shape[0]
        return full[t].at[pl.ds(pl.multiple_of(source * tall, tall), tall), :]

    def remote(source, target, send_sem, recv_sem, device):
        copy = pltpu.make_async_remote_copy(
            src_ref=source,
            dst_ref=target,
            send_sem=send_sem,
            recv_sem=recv_sem,
            device_id={"sp": device},
            device_id_type=MESH,
        )
        copy.start()
        return copy

    first, relays, local = {}, {}, {}
    for t in order:
        for d in range(1, nz):
            first[d, t] = remote(
                piece(t, places[d]), spot(t, me), send.at[d, t], recv.at[d, t], places[d] * 2 + c
            )
        relays[0, t] = remote(piece(t, z), spot(t, me), rsend.at[0, t], rrecv.at[0, t], partner)
        local[t] = pltpu.make_async_copy(piece(t, z), spot(t, me), own.at[t])
        local[t].start()

    def relay(d, t):
        source = lax.rem(z + nz - d, nz) * 2 + c
        first[d, t].wait_recv()
        relays[d, t] = remote(
            spot(t, source), spot(t, source), rsend.at[d, t], rrecv.at[d, t], partner
        )

    def arrive(t):
        local[t].wait()
        for d in range(nz):
            relays[d, t].wait_recv()

    group_arrays = lambda g: ([count - 1] if g == 0 else []) + [3 * g, 3 * g + 1, 3 * g + 2]
    for d in range(1, nz):
        for t in group_arrays(0):
            relay(d, t)

    tile = 2 * LANES
    upper = (
        lax.broadcasted_iota(jnp.int32, (tile, tile), 0)
        > lax.broadcasted_iota(jnp.int32, (tile, tile), 1)
    ).astype(jnp.bfloat16)
    lane = lax.broadcasted_iota(jnp.int32, (rows, LANES), 1)
    column = lax.broadcasted_iota(jnp.int32, (rows, tile), 1)
    line = lax.broadcasted_iota(jnp.int32, (rows, tile), 0)
    backs = []
    for g in range(g_count):
        units, size = groups[g]
        q_ref, k_ref, v_ref = full[3 * g : 3 * g + 3]
        r = n // units
        unit, j = me // r, lax.rem(me, r)
        heads = LANES // size
        scale = LOG2E * size ** (-0.5)
        for t in group_arrays(g):
            arrive(t)
        pending = []
        if g + 1 < g_count:
            pending = [(d, t) for d in range(1, nz) for t in group_arrays(g + 1)]
        for m in range(n // r):
            block = snake(r, j, m)
            last = lambda b: ((b + 1) * rows - 1) // tile
            counts = [last(snake(r, jj, m)) + 1 for jj in range(r)]
            query = q_ref[pl.ds(pl.multiple_of(block * rows, rows), rows), :]
            lines = ins[count - 1].shape[0]
            stop_t = full[count - 1][pl.ds(pl.multiple_of(block * lines, lines), lines), :]
            fill = jnp.zeros((LANES - lines, stop_t.shape[1]), jnp.float32)
            stop_all = jnp.concatenate([stop_t, fill], axis=0).T[:rows]
            parts = []
            for h in range(heads):
                head = offsets[g] + unit * heads + h
                stop = jnp.sum(jnp.where(lane == head, stop_all, 0.0), axis=1, keepdims=True) * LOG2E
                if heads > 1:
                    mine = query * ((lane // size) == h).astype(jnp.bfloat16)
                else:
                    mine = query
                carry = jnp.zeros((rows, 1), jnp.float32)
                total = jnp.zeros((rows, LANES), jnp.float32)
                for i in range(max(counts)):
                    where_tile = (block * rows + rows - 1) // tile - i
                    masked = i < 2 or i >= min(counts)
                    start = pl.multiple_of(jnp.maximum(where_tile, 0) * tile, tile)
                    keys = k_ref[pl.ds(start, tile), :]
                    values = v_ref[pl.ds(start, tile), :]
                    score = lax.dot_general(
                        mine, keys, (((1,), (1,)), ((), ())), preferred_element_type=jnp.float32
                    )
                    score = score * scale + stop
                    small = jnp.log2(1.0 + jnp.exp2(-jnp.abs(score)))
                    fail = jnp.maximum(score, 0.0) + small
                    hit = score - fail
                    if masked:
                        valid = column + where_tile * tile < line + block * rows
                        if i >= min(counts):
                            valid = jnp.logical_and(valid, where_tile >= 0)
                        fail = jnp.where(valid, fail, 0.0)
                    high = fail.astype(jnp.bfloat16)
                    low = (fail - high.astype(jnp.float32)).astype(jnp.bfloat16)
                    after = jnp.dot(high, upper, preferred_element_type=jnp.float32) + jnp.dot(
                        low, upper, preferred_element_type=jnp.float32
                    )
                    weight = jnp.exp2(hit - after - carry)
                    if masked:
                        weight = jnp.where(valid, weight, 0.0)
                    carry = carry + after[:, :1] + fail[:, :1]
                    total = total + jnp.dot(
                        weight.astype(jnp.bfloat16), values, preferred_element_type=jnp.float32
                    )
                parts.append(total)
            merged = parts[0]
            for h in range(1, heads):
                merged = jnp.where(lane // size >= h, parts[h], merged)
            made[g][m] = merged.astype(jnp.bfloat16)
            place = outs[g].at[:, pl.ds(pl.multiple_of(unit * LANES, LANES), LANES)]

            @pl.when(block != me)
            def _():
                pltpu.make_async_remote_copy(
                    src_ref=made[g].at[m],
                    dst_ref=place,
                    send_sem=bsend.at[g, m],
                    recv_sem=brecv.at[g, unit],
                    device_id={"sp": block},
                    device_id_type=MESH,
                ).start()

            @pl.when(block == me)
            def _():
                pltpu.make_async_copy(made[g].at[m], place, bsend.at[g, m]).start()

            share = -(-len(pending) // (n // r - m))
            for d, t in pending[:share]:
                relay(d, t)
            pending = pending[share:]

    for g in range(g_count):
        r = n // groups[g][0]
        turn, rest = me // r, lax.rem(me, r)
        owner = jnp.where(lax.rem(turn, 2) == 0, rest, r - 1 - rest)
        for u in range(groups[g][0]):

            @pl.when(u * r + owner != me)
            def _(g=g, u=u):
                place = outs[g].at[:, pl.ds(u * LANES, LANES)]
                pltpu.make_async_copy(place, place, brecv.at[g, u]).wait()

        unit = me // r
        place = outs[g].at[:, pl.ds(pl.multiple_of(unit * LANES, LANES), LANES)]
        for m in range(groups[g][0]):
            pltpu.make_async_copy(made[g].at[m], place, bsend.at[g, m]).wait()
    for copy in first.values():
        copy.wait_send()
    for copy in relays.values():
        copy.wait_send()


def stick(n, rows, arrays, groups, offsets, cid):
    k, g_count = len(arrays), len(groups)
    nz, top = n // 2, max(units for units, _ in groups)
    dma = pltpu.SemaphoreType.DMA
    return pl.pallas_call(
        functools.partial(stick_kernel, n, rows, groups, offsets),
        out_shape=tuple(
            jax.ShapeDtypeStruct((rows, units * LANES), jnp.bfloat16) for units, _ in groups
        ),
        in_specs=[VM] * k,
        out_specs=[VM] * g_count,
        scratch_shapes=[
            pltpu.VMEM((n * a.shape[0], LANES if i < k - 1 else a.shape[1]), a.dtype)
            for i, a in enumerate(arrays)
        ]
        + [pltpu.VMEM((units, rows, LANES), jnp.bfloat16) for units, _ in groups]
        + [dma((nz, k))] * 4
        + [dma((k,)), dma((g_count, top)), dma((g_count, top))],
        compiler_params=params(cid),
        name="stick",
    )(*arrays)


def exchange_kernel(axis, n, modes, *refs):
    count = len(modes)
    ins, outs = refs[:count], refs[count : 2 * count]
    send, recv = refs[2 * count :]
    me = lax.axis_index(axis)
    greet(axis, [lax.rem(me + d, n) for d in range(1, n)])

    def ends(t, peer):
        if modes[t] == "lead":
            return ins[t].at[peer], outs[t].at[me]
        if modes[t] == "cols":
            width = ins[t].shape[1] // n
            return ins[t].at[:, pl.ds(pl.multiple_of(peer * width, width), width)], outs[t].at[me]
        if modes[t] == "all":
            return ins[t], outs[t].at[me]
        width = ins[t].shape[1]
        return ins[t], outs[t].at[:, pl.ds(pl.multiple_of(me * width, width), width)]

    copies = []
    for d in range(1, n):
        peer = lax.rem(me + d, n)
        for t in range(count):
            source, target = ends(t, peer)
            copies.append(
                pltpu.make_async_remote_copy(
                    src_ref=source,
                    dst_ref=target,
                    send_sem=send.at[d, t],
                    recv_sem=recv.at[d, t],
                    device_id={axis: peer},
                    device_id_type=MESH,
                )
            )
            copies[-1].start()
    for t in range(count):
        source, target = ends(t, me)
        copies.append(pltpu.make_async_copy(source, target, send.at[0, t]))
        copies[-1].start()
    for copy in copies:
        copy.wait()


def exchange(axis, n, arrays, modes, cid):
    def shape(a, mode):
        if mode == "lead":
            return a.shape
        if mode == "cols":
            return (n, a.shape[0], a.shape[1] // n)
        if mode == "all":
            return (n,) + a.shape
        return (a.shape[0], a.shape[1] * n)

    if modes[0] == "cols" and any((a.shape[1] // n) % LANES for a in arrays):
        cut = [jnp.transpose(a.reshape(a.shape[0], n, -1), (1, 0, 2)) for a in arrays]
        return exchange(axis, n, cut, ("lead",) * len(cut), cid)
    if modes[0] == "side" and any(a.shape[1] % LANES for a in arrays):
        stacked = exchange(axis, n, arrays, ("all",) * len(arrays), cid)
        return [jnp.transpose(a, (1, 0, 2)).reshape(a.shape[1], -1) for a in stacked]
    k = len(arrays)
    return pl.pallas_call(
        functools.partial(exchange_kernel, axis, n, modes),
        out_shape=tuple(jax.ShapeDtypeStruct(shape(a, m), a.dtype) for a, m in zip(arrays, modes)),
        in_specs=[VM] * k,
        out_specs=[VM] * k,
        scratch_shapes=[pltpu.SemaphoreType.DMA((n, k))] * 2,
        compiler_params=params(cid),
        name="exchange",
    )(*arrays)


def flip(z, offset):
    other, bit = z, 1
    while bit <= offset:
        if offset & bit:
            other = other + bit - 2 * bit * lax.rem(z // bit, 2)
        bit *= 2
    return other


def layer_kernel(n_sp, n_tp, groups, capacity, order, *refs):
    f32, bf16 = jnp.float32, jnp.bfloat16
    pieces, refs = refs[:6], refs[6:]
    (stop_a, stop_b, routes_ref, gates_ref, mix_gain, ffn_gain), refs = refs[:6], refs[6:]
    large, refs = refs[:9], refs[9:]
    result_ref, refs = refs[0], refs[1:]
    full, refs = refs[:7], refs[7:]
    made, refs = refs[:2], refs[2:]
    attended, refs = refs[:2], refs[2:]
    held, refs = refs[:9], refs[9:]
    (stops_own, partial, part_out, part_in, aux, stats_out, stats_in, normed_ref), refs = (
        refs[:8],
        refs[8:],
    )
    (out_ref, arrived, returned, made_back, pre, pre_in, hid, s_pre, s_pre_in, s_hid), refs = (
        refs[:10],
        refs[10:],
    )
    (gather_ref, scatter_ref), refs = refs[:2], refs[2:]
    (load_sem, fsend, frecv, rsend, rrecv, osend, orecv, xsend, xrecv, tsend, trecv), refs = (
        refs[:11],
        refs[11:],
    )
    dsend, drecv, bsend, brecv, psend, precv, hsend, hrecv = refs

    me, col = lax.axis_index("sp"), lax.axis_index("tp")
    nz = n_sp // 2
    z, c = me // 2, lax.rem(me, 2)
    partner = z * 2 + 1 - c
    rows = pieces[0].shape[0]
    tall_rows = rows // LANES * LANES + (LANES if rows % LANES else 0)
    w_out_a, w_out_b, resid_ref, w_gate, w_up, w_down, sg_ref, su_ref, sd_ref = held
    experts = w_gate.shape[0]
    width = resid_ref.shape[1]
    block = arrived.shape[1]
    part = hid.shape[2] // n_tp

    def dot(a, b):
        return jnp.dot(a, b, preferred_element_type=f32)

    loads = [pltpu.make_async_copy(a, b, load_sem.at[i]) for i, (a, b) in enumerate(zip(large, held))]
    stops_own[...] = jnp.zeros_like(stops_own)
    heads_a, heads_b = stop_a.shape[0], stop_b.shape[0]
    stops_own[:heads_a, :rows] = stop_a[...]
    stops_own[heads_a : heads_a + heads_b, :rows] = stop_b[...]
    barrier = pltpu.get_barrier_semaphore()
    for d in range(1, n_sp):
        pl.semaphore_signal(
            barrier, inc=1, device_id={"sp": lax.rem(me + d, n_sp)}, device_id_type=MESH
        )
    for d in range(1, n_tp):
        pl.semaphore_signal(
            barrier, inc=1, device_id={"tp": lax.rem(col + d, n_tp)}, device_id_type=MESH
        )
    pl.semaphore_wait(barrier, n_sp + n_tp - 2)

    sends = []

    def remote(source, target, send, recv, where):
        copy = pltpu.make_async_remote_copy(
            src_ref=source,
            dst_ref=target,
            send_sem=send,
            recv_sem=recv,
            device_id=where,
            device_id_type=MESH,
        )
        copy.start()
        sends.append(copy)

    def landed(ref, sem):
        pltpu.make_async_copy(ref, ref, sem).wait()

    ins = tuple(pieces) + (stops_own,)
    names = ((6, 0, 1, 2), (3, 4, 5))

    def piece(t, place):
        if t == 6:
            return ins[t]
        return ins[t].at[:, pl.ds(pl.multiple_of(place * LANES, LANES), LANES)]

    def spot(t, source):
        tall = ins[t].shape[0]
        return full[t].at[pl.ds(pl.multiple_of(source * tall, tall), tall), :]

    places = [flip(z, o) for o in range(nz)]
    for g in range(2):
        for t in names[g]:
            for o in range(1, nz):
                remote(
                    piece(t, places[o]),
                    spot(t, me),
                    fsend.at[o, t],
                    frecv.at[z, t],
                    {"sp": places[o] * 2 + c},
                )
            pltpu.make_async_copy(piece(t, z), spot(t, me), frecv.at[z, t]).start()
    for load in loads:
        load.start()

    def relay(g, chip):
        for t in names[g]:
            mine = spot(t, chip * 2 + c)
            landed(mine, frecv.at[chip, t])
            remote(mine, mine, rsend.at[chip, t], rrecv.at[chip, t], {"sp": partner})

    def relayed(g, chip):
        for t in names[g]:
            landed(spot(t, chip * 2 + 1 - c), rrecv.at[chip, t])

    slot_rows = []

    def tables():
        total_experts = n_sp * experts
        kinds = lax.broadcasted_iota(jnp.int32, (total_experts, rows), 0)
        hots = [(kinds == routes_ref[t : t + 1, :]).astype(f32) for t in range(routes_ref.shape[0])]
        named = hots[0]
        for hot in hots[1:]:
            named = named + hot
        before = (
            lax.broadcasted_iota(jnp.int32, (rows, rows), 0)
            < lax.broadcasted_iota(jnp.int32, (rows, rows), 1)
        ).astype(bf16)
        earlier = dot(named.astype(bf16), before)
        aux[...] = jnp.zeros_like(aux)
        for t, hot in enumerate(hots):
            rank = jnp.sum(earlier * hot, axis=0, keepdims=True)
            slot = routes_ref[t : t + 1, :].astype(f32) * float(capacity) + rank
            slot_rows.append(slot)
            aux[t : t + 1, :rows] = slot
            aux[len(hots) + t : len(hots) + t + 1, :rows] = gates_ref[t : t + 1, :]
        spread = gather_ref.shape[0]
        tall = spread // experts

        def where_of(index, k):
            place = index + k * capacity
            for e in range(1, experts):
                place = place + jnp.where(index >= e * capacity, tall - capacity, 0)
            return place

        for k in range(2):
            index = lax.broadcasted_iota(jnp.int32, (spread, LANES), 1)
            hit = where_of(index, k) == lax.broadcasted_iota(jnp.int32, (spread, LANES), 0)
            hit = jnp.logical_and(hit, index < block)
            gather_ref[:, k * LANES : (k + 1) * LANES] = hit.astype(f32).astype(bf16)
            index = lax.broadcasted_iota(jnp.int32, (block, spread), 0)
            hit = where_of(index, k) == lax.broadcasted_iota(jnp.int32, (block, spread), 1)
            scatter_ref[k] = hit.astype(f32).astype(bf16)

    tile = 2 * LANES
    upper = (
        lax.broadcasted_iota(jnp.int32, (tile, tile), 0)
        > lax.broadcasted_iota(jnp.int32, (tile, tile), 1)
    ).astype(bf16)
    lane = lax.broadcasted_iota(jnp.int32, (rows, LANES), 1)
    column = lax.broadcasted_iota(jnp.int32, (rows, tile), 1)
    line = lax.broadcasted_iota(jnp.int32, (rows, tile), 0)

    backs = []
    steps = [(g, m) for g in range(2) for m in range(nz)]
    offsets = (0, heads_a)
    relay(0, 0)
    tables()
    relayed(0, 0)
    for number, (g, m) in enumerate(steps):
        size = groups[g][1]
        heads = LANES // size
        q_ref, k_ref, v_ref = full[3 * g : 3 * g + 3]
        scale = LOG2E * size ** (-0.5)
        block_q = 2 * m + (c if m % 2 == 0 else 1 - c)
        count = -(-(2 * m + 2) * rows // tile)
        query = q_ref[pl.ds(pl.multiple_of(block_q * rows, rows), rows), :]
        lines = stops_own.shape[0]
        stop_t = full[6][pl.ds(pl.multiple_of(block_q * lines, lines), lines), :]
        fill = jnp.zeros((LANES - lines, stop_t.shape[1]), f32)
        stop_all = jnp.concatenate([stop_t, fill], axis=0).T[:rows]
        parts = []
        for h in range(heads):
            head = offsets[g] + z * heads + h
            stop = jnp.sum(jnp.where(lane == head, stop_all, 0.0), axis=1, keepdims=True) * LOG2E
            mine = query * ((lane // size) == h).astype(bf16) if heads > 1 else query
            carry = jnp.zeros((rows, 1), f32)
            total = jnp.zeros((rows, LANES), f32)
            for i in range(count):
                if h == heads - 1 and i == count // 2 and number + 1 < len(steps):
                    relay(*steps[number + 1])
                begin = block_q * rows + rows - tile * (i + 1)
                short = (2 * m + 1) * rows - tile * (i + 1) < 0
                short = short or (2 * m + 2) * rows - tile * (i + 1) < 0
                masked = i == 0 or short
                start = pl.multiple_of(jnp.maximum(begin, 0), math.gcd(rows, tile))
                keys = k_ref[pl.ds(start, tile), :]
                values = v_ref[pl.ds(start, tile), :]
                score = lax.dot_general(
                    mine, keys, (((1,), (1,)), ((), ())), preferred_element_type=f32
                )
                score = score * scale + stop
                small = jnp.log2(1.0 + jnp.exp2(-jnp.abs(score)))
                fail = jnp.maximum(score, 0.0) + small
                hit = score - fail
                if masked:
                    valid = column < begin + tile - start
                    if i == 0:
                        valid = column + start < line + block_q * rows
                    fail = jnp.where(valid, fail, 0.0)
                high = fail.astype(bf16)
                low = (fail - high.astype(f32)).astype(bf16)
                after = dot(high, upper) + dot(low, upper)
                weight = jnp.exp2(hit - after - carry)
                if masked:
                    weight = jnp.where(valid, weight, 0.0)
                carry = carry + after[:, :1] + fail[:, :1]
                total = total + dot(weight.astype(bf16), values)
            parts.append(total)
        merged = parts[0]
        for h in range(1, heads):
            merged = jnp.where(lane // size >= h, parts[h], merged)
        made[g][m] = merged.astype(bf16)
        place = attended[g].at[:, pl.ds(pl.multiple_of(z * LANES, LANES), LANES)]
        backs.append((g, m, block_q))

        @pl.when(block_q != me)
        def _(g=g, m=m, place=place, block_q=block_q):
            pltpu.make_async_remote_copy(
                src_ref=made[g].at[m],
                dst_ref=place,
                send_sem=osend.at[g, m],
                recv_sem=orecv.at[g, z],
                device_id={"sp": block_q},
                device_id_type=MESH,
            ).start()

        @pl.when(block_q == me)
        def _(g=g, m=m, place=place):
            pltpu.make_async_copy(made[g].at[m], place, orecv.at[g, z]).start()

        if number + 1 < len(steps):
            relayed(*steps[number + 1])

    loads[0].wait()
    loads[1].wait()
    loads[2].wait()

    def columns(which, wide):
        return pl.ds(pl.multiple_of(which * wide, wide), wide)

    peers = [lax.rem(col + d, n_tp) for d in range(1, n_tp)] + [col]
    for g, weights in enumerate((w_out_a, w_out_b)):
        for u in range(groups[g][0]):
            landed(attended[g].at[:, u * LANES : (u + 1) * LANES], orecv.at[g, u])
        left = attended[g][...]
        for i, peer in enumerate(peers):
            term = dot(left, weights[:, columns(peer, width)])
            if g == 0:
                partial[i] = term
                continue
            part_out[i] = (partial[i] + term).astype(bf16)
            if i < n_tp - 1:
                remote(part_out.at[i], part_in.at[i], xsend.at[i], xrecv.at[i], {"tp": peer})
    resid = resid_ref[...].astype(f32)
    mixed = part_out[n_tp - 1].astype(f32)
    for i in range(n_tp - 1):
        landed(part_in.at[i], xrecv.at[i])
        mixed = mixed + part_in[i].astype(f32)

    shaped = mixed * mix_gain[...]
    sums = jnp.zeros((rows, LANES), f32)
    for i, term in enumerate((mixed * mixed, resid * resid, resid * shaped, shaped * shaped)):
        sums = jnp.where(lane == i, jnp.sum(term, axis=1, keepdims=True), sums)
    if tall_rows > rows:
        sums = jnp.concatenate([sums, jnp.zeros((tall_rows - rows, LANES), f32)], axis=0)
    stats_out[...] = sums.T[:8]
    for d in range(1, n_tp):
        remote(
            stats_out, stats_in.at[d - 1], tsend.at[d - 1], trecv.at[d - 1], {"tp": peers[d - 1]}
        )
    sums = stats_out[...]
    for d in range(1, n_tp):
        landed(stats_in.at[d - 1], trecv.at[d - 1])
        sums = sums + stats_in[d - 1]
    sums = jnp.concatenate([sums, jnp.zeros((LANES - 8, tall_rows), f32)], axis=0).T[:rows]
    model = width * n_tp
    scale = lax.rsqrt(sums[:, 0:1] / model + epsilon)
    stream = (resid + shaped * scale).astype(bf16)
    square = sums[:, 1:2] + scale * (2.0 * sums[:, 2:3] + scale * sums[:, 3:4])
    square = jnp.maximum(square, 0.0)
    stream = stream.astype(f32)
    result_ref[...] = stream
    normed = stream * lax.rsqrt(square / model + epsilon) * ffn_gain[...]
    normed_ref[...] = normed.astype(bf16)

    chips = [flip(z, o) for o in order]
    shared = len(chips)
    seat = lax.broadcasted_iota(jnp.int32, (block, rows), 0)
    for i, o in enumerate(order):
        for k in range(2):
            peer = chips[i] * 2 + lax.rem(c + k, 2)
            seats = (seat + peer * block).astype(f32)
            chosen = seats == slot_rows[0]
            for slot in slot_rows[1:]:
                chosen = jnp.logical_or(chosen, seats == slot)
            picked = dot(chosen.astype(f32).astype(bf16), normed_ref[...])
            out_ref[2 * i + k] = picked.astype(bf16)
            if o == 0 and k == 0:
                pltpu.make_async_copy(out_ref.at[2 * i + k], arrived.at[me], drecv.at[me]).start()
            else:
                remote(
                    out_ref.at[2 * i + k],
                    arrived.at[me],
                    dsend.at[2 * i + k],
                    drecv.at[me],
                    {"sp": peer},
                )

    def buffers(i):
        if i == shared:
            return s_pre, s_pre_in, s_hid
        return pre.at[i], pre_in.at[i], hid.at[i]

    def first(i):
        here, there, _ = buffers(i)
        if i == shared:
            loads[6].wait()
            loads[7].wait()
            for k, weight in enumerate((sg_ref, su_ref)):
                here[k] = dot(normed_ref[...], weight[...]).astype(bf16)
        else:
            grouped = None
            for k in range(2):
                source = chips[i] * 2 + k
                landed(arrived.at[source], drecv.at[source])
                term = dot(gather_ref[:, k * LANES : k * LANES + block], arrived[source])
                grouped = term if grouped is None else grouped + term
            grouped = grouped.astype(bf16)
            tall = grouped.shape[0] // experts
            if i == 0:
                loads[3].wait()
                loads[4].wait()
            for k, weight in enumerate((w_gate, w_up)):
                terms = [
                    dot(grouped[e * tall : (e + 1) * tall], weight[e]).astype(bf16)
                    for e in range(experts)
                ]
                spread_rows = jnp.concatenate(terms, axis=0)
                here[k] = jnp.concatenate(
                    [dot(scatter_ref[j], spread_rows) for j in range(2)], axis=0
                ).astype(bf16)
        for d in range(1, n_tp):
            for k in range(2):
                remote(
                    here.at[k, :, columns(peers[d - 1], part)],
                    there.at[d - 1, k],
                    psend.at[i, d - 1, k],
                    precv.at[i, d - 1, k],
                    {"tp": peers[d - 1]},
                )

    def second(i):
        here, there, whole = buffers(i)
        sums = []
        for k in range(2):
            total = here[k, :, columns(col, part)].astype(f32)
            for d in range(1, n_tp):
                landed(there.at[d - 1, k], precv.at[i, d - 1, k])
                total = total + there[d - 1, k].astype(f32)
            sums.append(total)
        whole[:, columns(col, part)] = (sums[0] / (1.0 + jnp.exp(-sums[0])) * sums[1]).astype(bf16)
        for d in range(1, n_tp):
            mine = whole.at[:, columns(col, part)]
            remote(mine, mine, hsend.at[i, d - 1], hrecv.at[i, d - 1], {"tp": peers[d - 1]})

    kept = []

    def third(i):
        _, _, whole = buffers(i)
        for d in range(1, n_tp):
            source = lax.rem(col + n_tp - d, n_tp)
            landed(whole.at[:, columns(source, part)], hrecv.at[i, d - 1])
        if i == shared:
            loads[8].wait()
            result_ref[...] = result_ref[...] + dot(whole[...], sd_ref[...])
            return
        hidden = whole[...]
        grouped = dot(gather_ref[:, :block], hidden[:block]) + dot(
            gather_ref[:, LANES : LANES + block], hidden[block:]
        )
        grouped = grouped.astype(bf16)
        tall = grouped.shape[0] // experts
        if i == 0:
            loads[5].wait()
        terms = [
            dot(grouped[e * tall : (e + 1) * tall], w_down[e]).astype(bf16) for e in range(experts)
        ]
        terms = jnp.concatenate(terms, axis=0)
        for k in range(2):
            source = chips[i] * 2 + k
            made_back[i, k] = dot(scatter_ref[k], terms).astype(bf16)
            if order[i] == 0:

                @pl.when(source != me)
                def _():
                    pltpu.make_async_remote_copy(
                        src_ref=made_back.at[i, k],
                        dst_ref=returned.at[me],
                        send_sem=bsend.at[i, k],
                        recv_sem=brecv.at[me],
                        device_id={"sp": source},
                        device_id_type=MESH,
                    ).start()

                @pl.when(source == me)
                def _():
                    pltpu.make_async_copy(made_back.at[i, k], returned.at[me], brecv.at[me]).start()

                kept.append((i, k, source))
            else:
                remote(
                    made_back.at[i, k],
                    returned.at[me],
                    bsend.at[i, k],
                    brecv.at[me],
                    {"sp": source},
                )

    top_count = routes_ref.shape[0]
    turned = aux[...].T[:rows]
    taken = lax.broadcasted_iota(jnp.int32, (rows, block), 1)

    def combine(i):
        total = result_ref[...]
        for k in range(2):
            source = chips[i] * 2 + k
            landed(returned.at[source], brecv.at[source])
            seats = (taken + source * block).astype(f32)
            gated = jnp.zeros(seats.shape, f32)
            for t in range(top_count):
                gate = turned[:, top_count + t : top_count + t + 1]
                gated = gated + jnp.where(seats == turned[:, t : t + 1], gate, 0.0)
            high = gated.astype(bf16)
            low = (gated - high.astype(f32)).astype(bf16)
            total = total + dot(high, returned[source]) + dot(low, returned[source])
        result_ref[...] = total

    first(shared)
    first(0)
    second(shared)
    for i in range(1, shared + 2):
        if i < shared:
            first(i)
        if i <= shared:
            second(i - 1)
        if i == 1:
            third(shared)
        else:
            third(i - 2)
    for i in range(shared):
        combine(i)
    for copy in sends:
        copy.wait_send()
    for g, m, block_q in backs:

        @pl.when(block_q != me)
        def _(g=g, m=m):
            landed(made[g].at[m], osend.at[g, m])

    for i, k, source in kept:

        @pl.when(source != me)
        def _(i=i, k=k):
            landed(made_back.at[i, k], bsend.at[i, k])


def layer(n_sp, n_tp, groups, capacity, arrays, small, large):
    f32, bf16 = jnp.float32, jnp.bfloat16
    rows = arrays[0].shape[0]
    resid, w_gate = large[2], large[3]
    width = resid.shape[1]
    experts, hidden_width = w_gate.shape[0], w_gate.shape[2]
    block = experts * capacity
    nz = n_sp // 2
    order = (0,) + tuple(range(nz - 1, 0, -1))
    wide = -(-rows // LANES) * LANES
    lines = -(-(small[0].shape[0] + small[1].shape[0]) // 8) * 8
    tall = -(-2 * capacity // 16) * 16
    part = hidden_width // n_tp
    dma = pltpu.SemaphoreType.DMA
    vmem = pltpu.VMEM
    anywhere = pl.BlockSpec(memory_space=pl.ANY)
    scratch = (
        [vmem((n_sp * rows, LANES), bf16)] * 6
        + [vmem((n_sp * lines, wide), f32)]
        + [vmem((nz, rows, LANES), bf16)] * 2
        + [vmem((rows, units * LANES), bf16) for units, _ in groups]
        + [vmem(a.shape, a.dtype) for a in large]
        + [
            vmem((lines, wide), f32),
            vmem((n_tp, rows, width), f32),
            vmem((n_tp, rows, width), bf16),
            vmem((n_tp - 1, rows, width), bf16),
            vmem((LANES, wide), f32),
            vmem((8, wide), f32),
            vmem((n_tp - 1, 8, wide), f32),
            vmem((rows, width), bf16),
        ]
        + [
            vmem((n_sp, block, width), bf16),
            vmem((n_sp, block, width), bf16),
            vmem((n_sp, block, width), bf16),
            vmem((nz, 2, block, width), bf16),
            vmem((nz, 2, 2 * block, hidden_width), bf16),
            vmem((nz, n_tp - 1, 2, 2 * block, part), bf16),
            vmem((nz, 2 * block, hidden_width), bf16),
            vmem((2, rows, hidden_width), bf16),
            vmem((n_tp - 1, 2, rows, part), bf16),
            vmem((rows, hidden_width), bf16),
        ]
        + [vmem((experts * tall, 2 * LANES), bf16), vmem((2, block, experts * tall), bf16)]
        + [dma((len(large),))]
        + [dma((nz, 7))] * 4
        + [dma((2, nz))] * 2
        + [dma((n_tp - 1,))] * 4
        + [dma((n_sp,)), dma((n_sp,)), dma((nz, 2)), dma((n_sp,))]
        + [dma((nz + 1, n_tp - 1, 2))] * 2
        + [dma((nz + 1, n_tp - 1))] * 2
    )
    return pl.pallas_call(
        functools.partial(layer_kernel, n_sp, n_tp, groups, capacity, order),
        out_shape=jax.ShapeDtypeStruct((rows, width), f32),
        in_specs=[VM] * 12 + [anywhere] * 9,
        out_specs=VM,
        scratch_shapes=scratch,
        compiler_params=params(9),
        name="layer",
    )(*arrays, *small, *large)


def shards(
    n_sp,
    n_tp,
    query_a,
    key_a,
    value_a,
    query_b,
    key_b,
    value_b,
    stop_a,
    stop_b,
    out_a,
    out_b,
    resid,
    mix_gain,
    ffn_gain,
    routes,
    gates,
    exp_gate,
    exp_up,
    exp_down,
    sh_gate,
    sh_up,
    sh_down,
):
    f32, bf16 = jnp.float32, jnp.bfloat16
    rows = query_a.shape[0]
    heads_a, heads_b = stop_a.shape[1], stop_b.shape[1]
    units_a, units_b = query_a.shape[1] // LANES, query_b.shape[1] // LANES
    width = resid.shape[1]
    model = width * n_tp

    local_experts = exp_gate.shape[0]
    experts = local_experts * n_sp
    top_count = routes.shape[1]
    capacity = max(1, (3 * rows * top_count + 2 * experts - 1) // (2 * experts))
    block = local_experts * capacity
    hidden_width = exp_gate.shape[2]
    groups = ((units_a, query_a.shape[1] // heads_a), (units_b, query_b.shape[1] // heads_b))
    fused = (
        (hidden_width // n_tp) % LANES == 0
        and width % LANES == 0
        and block % 8 == 0
        and block <= LANES
        and exp_gate.shape == exp_down.shape
        and all(2 * units == n_sp for units, _ in groups)
        and (n_sp // 2) & (n_sp // 2 - 1) == 0
        and 2 * rows <= 4 * LANES
    )
    if fused:
        arrays = (query_a, key_a, value_a, query_b, key_b, value_b)
        small = (stop_a.T, stop_b.T, routes.T, gates.T, mix_gain[None, :], ffn_gain[None, :])
        large = (out_a, out_b, resid, exp_gate, exp_up, exp_down, sh_gate, sh_up, sh_down)
        return layer(n_sp, n_tp, groups, capacity, arrays, small, large).astype(bf16)

    flat_routes = routes.reshape(-1)
    onehot = (flat_routes[:, None] == jnp.arange(experts, dtype=jnp.int32)[None, :]).astype(f32)
    pairs = rows * top_count
    before = (jnp.arange(pairs)[:, None] > jnp.arange(pairs)[None, :]).astype(bf16)
    earlier = jnp.dot(before, onehot.astype(bf16), preferred_element_type=f32)
    slot = flat_routes * capacity + jnp.sum(earlier * onehot, axis=1).astype(jnp.int32)
    slot = slot.reshape(rows, top_count)
    slots = jnp.arange(experts * capacity, dtype=jnp.int32)
    chosen = slot[:, :, None] == slots[None, None, :]
    chooser = jnp.sum(chosen.astype(f32), axis=1).astype(bf16)
    gated = jnp.sum(jnp.where(chosen, gates[:, :, None], 0.0), axis=1)
    gated_high = gated.astype(bf16)
    gated_low = (gated - gated_high.astype(f32)).astype(bf16)

    stops = jnp.concatenate([stop_a, stop_b], axis=1)
    lines = -(-stops.shape[1] // 8) * 8
    wide = -(-rows // LANES) * LANES
    stops = jnp.pad(stops.T, ((0, lines - stops.shape[1]), (0, wide - rows)))
    arrays = (query_a, key_a, value_a, query_b, key_b, value_b, stops)
    attended_a, attended_b = stick(n_sp, rows, arrays, groups, (0, heads_a), 0)

    partial_value = jnp.dot(attended_a, out_a, preferred_element_type=f32)
    partial_value = partial_value + jnp.dot(attended_b, out_b, preferred_element_type=f32)
    (pieces,) = exchange("tp", n_tp, (partial_value.astype(bf16),), ("cols",), 2)
    mixed = jnp.sum(pieces.astype(f32), axis=0)
    resid_f = resid.astype(f32)
    shaped = mixed * mix_gain[None, :]
    sums = jnp.stack(
        [
            jnp.sum(mixed * mixed, axis=1),
            jnp.sum(resid_f * resid_f, axis=1),
            jnp.sum(resid_f * shaped, axis=1),
            jnp.sum(shaped * shaped, axis=1),
        ]
    )
    sums = jnp.pad(sums, ((0, 4), (0, wide - rows)))
    (sums,) = exchange("tp", n_tp, (sums,), ("all",), 3)
    sums = jnp.sum(sums, axis=0)[:4, :rows]
    scale = lax.rsqrt(sums[0] / model + epsilon)
    stream = (resid_f + shaped * scale[:, None]).astype(bf16)
    square = jnp.maximum(sums[1] + scale * (2.0 * sums[2] + scale * sums[3]), 0.0)
    stream_f = stream.astype(f32)
    normed = (stream_f * lax.rsqrt(square / model + epsilon)[:, None] * ffn_gain[None, :]).astype(bf16)

    outgoing = lax.dot_general(chooser, normed, (((0,), (0,)), ((), ())), preferred_element_type=f32)
    outgoing = outgoing.astype(bf16).reshape(n_sp, local_experts * capacity, width)
    (arrived,) = exchange("sp", n_sp, (outgoing,), ("lead",), 4)
    arrived = arrived.reshape(n_sp, local_experts, capacity, width)
    arrived = jnp.transpose(arrived, (1, 0, 2, 3)).reshape(local_experts, n_sp * capacity, width)

    shared_parts = [
        jnp.dot(normed, w, preferred_element_type=f32).astype(bf16) for w in (sh_gate, sh_up)
    ]
    expert_parts = [
        jnp.einsum("erd,edf->erf", arrived, w, preferred_element_type=f32)
        .astype(bf16)
        .reshape(local_experts * n_sp * capacity, -1)
        for w in (exp_gate, exp_up)
    ]
    parts = exchange("tp", n_tp, (*expert_parts, *shared_parts), ("cols",) * 4, 5)
    gate_pre, up_pre, shared_gate, shared_up = [jnp.sum(p.astype(f32), axis=0) for p in parts]
    hidden = (jax.nn.silu(gate_pre) * up_pre).astype(bf16)
    shared_hidden = (jax.nn.silu(shared_gate) * shared_up).astype(bf16)
    hidden, shared_hidden = exchange("tp", n_tp, (hidden, shared_hidden), ("side",) * 2, 6)

    shared_out = jnp.dot(shared_hidden, sh_down, preferred_element_type=f32)
    hidden = hidden.reshape(local_experts, n_sp * capacity, -1)
    produced = jnp.einsum("erf,efd->erd", hidden, exp_down, preferred_element_type=f32).astype(bf16)
    produced = produced.reshape(local_experts, n_sp, capacity, width)
    produced = jnp.transpose(produced, (1, 0, 2, 3)).reshape(n_sp, local_experts * capacity, width)
    (returned,) = exchange("sp", n_sp, (produced,), ("lead",), 7)
    flat_back = returned.reshape(experts * capacity, width)
    routed = jnp.dot(gated_high, flat_back, preferred_element_type=f32)
    routed = routed + jnp.dot(gated_low, flat_back, preferred_element_type=f32)
    moe = routed + shared_out
    return (stream_f + moe).astype(bf16)


def solution(mesh):
    return jax.shard_map(
        functools.partial(shards, mesh.shape["sp"], mesh.shape["tp"]),
        mesh=mesh,
        in_specs=(
            P("sp", "tp"),
            P("sp", "tp"),
            P("sp", "tp"),
            P("sp", "tp"),
            P("sp", "tp"),
            P("sp", "tp"),
            P("sp", "tp"),
            P("sp", "tp"),
            P("tp", None),
            P("tp", None),
            P("sp", "tp"),
            P("tp"),
            P("tp"),
            P("sp", None),
            P("sp", None),
            P("sp", "tp", None),
            P("sp", "tp", None),
            P("sp", None, "tp"),
            P("tp", None),
            P("tp", None),
            P(None, "tp"),
        ),
        out_specs=P("sp", "tp"),
        check_vma=False,
    )
```

```python
import functools
import math

import jax
import jax.numpy as jnp
import numpy as np
from jax import lax
from jax.experimental import pallas as pl
from jax.experimental.pallas import tpu as pltpu
from jax.sharding import PartitionSpec as P

MESH = pl.DeviceIdType.MESH
LANES = 128
LOG2E = 1.4426950408889634
epsilon = 1e-06
VM = pl.BlockSpec(memory_space=pltpu.VMEM)


def greet(axis, peers):
    barrier = pltpu.get_barrier_semaphore()
    for peer in peers:
        pl.semaphore_signal(barrier, inc=1, device_id={axis: peer}, device_id_type=MESH)
    pl.semaphore_wait(barrier, len(peers))


def params(cid):
    return pltpu.CompilerParams(
        collective_id=cid, has_side_effects=True, vmem_limit_bytes=56 * 1024 * 1024
    )


def snake(r, j, m):
    return m * r + (j if m % 2 == 0 else r - 1 - j)


def stick_kernel(n, rows, groups, offsets, *refs):
    g_count = len(groups)
    count = 3 * g_count + 1
    ins, outs = refs[:count], refs[count : count + g_count]
    full = refs[count + g_count : 2 * count + g_count]
    made = refs[2 * count + g_count : 2 * count + 2 * g_count]
    send, recv, rsend, rrecv, own, bsend, brecv = refs[2 * count + 2 * g_count :]
    me = lax.axis_index("sp")
    nz = n // 2
    z, c = me // 2, lax.rem(me, 2)
    partner = z * 2 + 1 - c
    places = [lax.rem(z + d, nz) for d in range(nz)]
    greet("sp", [lax.rem(me + d, n) for d in range(1, n)])
    order = [count - 1] + list(range(count - 1))

    def piece(t, place):
        if t == count - 1:
            return ins[t]
        unit = (2 * place) // (n // groups[t // 3][0])
        return ins[t].at[:, pl.ds(pl.multiple_of(unit * LANES, LANES), LANES)]

    def spot(t, source):
        tall = ins[t].shape[0]
        return full[t].at[pl.ds(pl.multiple_of(source * tall, tall), tall), :]

    def remote(source, target, send_sem, recv_sem, device):
        copy = pltpu.make_async_remote_copy(
            src_ref=source,
            dst_ref=target,
            send_sem=send_sem,
            recv_sem=recv_sem,
            device_id={"sp": device},
            device_id_type=MESH,
        )
        copy.start()
        return copy

    first, relays, local = {}, {}, {}
    for t in order:
        for d in range(1, nz):
            first[d, t] = remote(
                piece(t, places[d]), spot(t, me), send.at[d, t], recv.at[d, t], places[d] * 2 + c
            )
        relays[0, t] = remote(piece(t, z), spot(t, me), rsend.at[0, t], rrecv.at[0, t], partner)
        local[t] = pltpu.make_async_copy(piece(t, z), spot(t, me), own.at[t])
        local[t].start()

    def relay(d, t):
        source = lax.rem(z + nz - d, nz) * 2 + c
        first[d, t].wait_recv()
        relays[d, t] = remote(
            spot(t, source), spot(t, source), rsend.at[d, t], rrecv.at[d, t], partner
        )

    def arrive(t):
        local[t].wait()
        for d in range(nz):
            relays[d, t].wait_recv()

    group_arrays = lambda g: ([count - 1] if g == 0 else []) + [3 * g, 3 * g + 1, 3 * g + 2]
    for d in range(1, nz):
        for t in group_arrays(0):
            relay(d, t)

    tile = 2 * LANES
    upper = (
        lax.broadcasted_iota(jnp.int32, (tile, tile), 0)
        > lax.broadcasted_iota(jnp.int32, (tile, tile), 1)
    ).astype(jnp.bfloat16)
    lane = lax.broadcasted_iota(jnp.int32, (rows, LANES), 1)
    column = lax.broadcasted_iota(jnp.int32, (rows, tile), 1)
    line = lax.broadcasted_iota(jnp.int32, (rows, tile), 0)
    backs = []
    for g in range(g_count):
        units, size = groups[g]
        q_ref, k_ref, v_ref = full[3 * g : 3 * g + 3]
        r = n // units
        unit, j = me // r, lax.rem(me, r)
        heads = LANES // size
        scale = LOG2E * size ** (-0.5)
        for t in group_arrays(g):
            arrive(t)
        pending = []
        if g + 1 < g_count:
            pending = [(d, t) for d in range(1, nz) for t in group_arrays(g + 1)]
        for m in range(n // r):
            block = snake(r, j, m)
            last = lambda b: ((b + 1) * rows - 1) // tile
            counts = [last(snake(r, jj, m)) + 1 for jj in range(r)]
            query = q_ref[pl.ds(pl.multiple_of(block * rows, rows), rows), :]
            lines = ins[count - 1].shape[0]
            stop_t = full[count - 1][pl.ds(pl.multiple_of(block * lines, lines), lines), :]
            fill = jnp.zeros((LANES - lines, stop_t.shape[1]), jnp.float32)
            stop_all = jnp.concatenate([stop_t, fill], axis=0).T[:rows]
            parts = []
            for h in range(heads):
                head = offsets[g] + unit * heads + h
                stop = jnp.sum(jnp.where(lane == head, stop_all, 0.0), axis=1, keepdims=True) * LOG2E
                if heads > 1:
                    mine = query * ((lane // size) == h).astype(jnp.bfloat16)
                else:
                    mine = query
                carry = jnp.zeros((rows, 1), jnp.float32)
                total = jnp.zeros((rows, LANES), jnp.float32)
                for i in range(max(counts)):
                    where_tile = (block * rows + rows - 1) // tile - i
                    masked = i < 2 or i >= min(counts)
                    start = pl.multiple_of(jnp.maximum(where_tile, 0) * tile, tile)
                    keys = k_ref[pl.ds(start, tile), :]
                    values = v_ref[pl.ds(start, tile), :]
                    score = lax.dot_general(
                        mine, keys, (((1,), (1,)), ((), ())), preferred_element_type=jnp.float32
                    )
                    score = score * scale + stop
                    small = jnp.log2(1.0 + jnp.exp2(-jnp.abs(score)))
                    fail = jnp.maximum(score, 0.0) + small
                    hit = score - fail
                    if masked:
                        valid = column + where_tile * tile < line + block * rows
                        if i >= min(counts):
                            valid = jnp.logical_and(valid, where_tile >= 0)
                        fail = jnp.where(valid, fail, 0.0)
                    high = fail.astype(jnp.bfloat16)
                    low = (fail - high.astype(jnp.float32)).astype(jnp.bfloat16)
                    after = jnp.dot(high, upper, preferred_element_type=jnp.float32) + jnp.dot(
                        low, upper, preferred_element_type=jnp.float32
                    )
                    weight = jnp.exp2(hit - after - carry)
                    if masked:
                        weight = jnp.where(valid, weight, 0.0)
                    carry = carry + after[:, :1] + fail[:, :1]
                    total = total + jnp.dot(
                        weight.astype(jnp.bfloat16), values, preferred_element_type=jnp.float32
                    )
                parts.append(total)
            merged = parts[0]
            for h in range(1, heads):
                merged = jnp.where(lane // size >= h, parts[h], merged)
            made[g][m] = merged.astype(jnp.bfloat16)
            place = outs[g].at[:, pl.ds(pl.multiple_of(unit * LANES, LANES), LANES)]

            @pl.when(block != me)
            def _():
                pltpu.make_async_remote_copy(
                    src_ref=made[g].at[m],
                    dst_ref=place,
                    send_sem=bsend.at[g, m],
                    recv_sem=brecv.at[g, unit],
                    device_id={"sp": block},
                    device_id_type=MESH,
                ).start()

            @pl.when(block == me)
            def _():
                pltpu.make_async_copy(made[g].at[m], place, bsend.at[g, m]).start()

            share = -(-len(pending) // (n // r - m))
            for d, t in pending[:share]:
                relay(d, t)
            pending = pending[share:]

    for g in range(g_count):
        r = n // groups[g][0]
        turn, rest = me // r, lax.rem(me, r)
        owner = jnp.where(lax.rem(turn, 2) == 0, rest, r - 1 - rest)
        for u in range(groups[g][0]):

            @pl.when(u * r + owner != me)
            def _(g=g, u=u):
                place = outs[g].at[:, pl.ds(u * LANES, LANES)]
                pltpu.make_async_copy(place, place, brecv.at[g, u]).wait()

        unit = me // r
        place = outs[g].at[:, pl.ds(pl.multiple_of(unit * LANES, LANES), LANES)]
        for m in range(groups[g][0]):
            pltpu.make_async_copy(made[g].at[m], place, bsend.at[g, m]).wait()
    for copy in first.values():
        copy.wait_send()
    for copy in relays.values():
        copy.wait_send()


def stick(n, rows, arrays, groups, offsets, cid):
    k, g_count = len(arrays), len(groups)
    nz, top = n // 2, max(units for units, _ in groups)
    dma = pltpu.SemaphoreType.DMA
    return pl.pallas_call(
        functools.partial(stick_kernel, n, rows, groups, offsets),
        out_shape=tuple(
            jax.ShapeDtypeStruct((rows, units * LANES), jnp.bfloat16) for units, _ in groups
        ),
        in_specs=[VM] * k,
        out_specs=[VM] * g_count,
        scratch_shapes=[
            pltpu.VMEM((n * a.shape[0], LANES if i < k - 1 else a.shape[1]), a.dtype)
            for i, a in enumerate(arrays)
        ]
        + [pltpu.VMEM((units, rows, LANES), jnp.bfloat16) for units, _ in groups]
        + [dma((nz, k))] * 4
        + [dma((k,)), dma((g_count, top)), dma((g_count, top))],
        compiler_params=params(cid),
        name="stick",
    )(*arrays)


def exchange_kernel(axis, n, modes, *refs):
    count = len(modes)
    ins, outs = refs[:count], refs[count : 2 * count]
    send, recv = refs[2 * count :]
    me = lax.axis_index(axis)
    greet(axis, [lax.rem(me + d, n) for d in range(1, n)])

    def ends(t, peer):
        if modes[t] == "lead":
            return ins[t].at[peer], outs[t].at[me]
        if modes[t] == "cols":
            width = ins[t].shape[1] // n
            return ins[t].at[:, pl.ds(pl.multiple_of(peer * width, width), width)], outs[t].at[me]
        if modes[t] == "all":
            return ins[t], outs[t].at[me]
        width = ins[t].shape[1]
        return ins[t], outs[t].at[:, pl.ds(pl.multiple_of(me * width, width), width)]

    copies = []
    for d in range(1, n):
        peer = lax.rem(me + d, n)
        for t in range(count):
            source, target = ends(t, peer)
            copies.append(
                pltpu.make_async_remote_copy(
                    src_ref=source,
                    dst_ref=target,
                    send_sem=send.at[d, t],
                    recv_sem=recv.at[d, t],
                    device_id={axis: peer},
                    device_id_type=MESH,
                )
            )
            copies[-1].start()
    for t in range(count):
        source, target = ends(t, me)
        copies.append(pltpu.make_async_copy(source, target, send.at[0, t]))
        copies[-1].start()
    for copy in copies:
        copy.wait()


def exchange(axis, n, arrays, modes, cid):
    def shape(a, mode):
        if mode == "lead":
            return a.shape
        if mode == "cols":
            return (n, a.shape[0], a.shape[1] // n)
        if mode == "all":
            return (n,) + a.shape
        return (a.shape[0], a.shape[1] * n)

    if modes[0] == "cols" and any((a.shape[1] // n) % LANES for a in arrays):
        cut = [jnp.transpose(a.reshape(a.shape[0], n, -1), (1, 0, 2)) for a in arrays]
        return exchange(axis, n, cut, ("lead",) * len(cut), cid)
    if modes[0] == "side" and any(a.shape[1] % LANES for a in arrays):
        stacked = exchange(axis, n, arrays, ("all",) * len(arrays), cid)
        return [jnp.transpose(a, (1, 0, 2)).reshape(a.shape[1], -1) for a in stacked]
    k = len(arrays)
    return pl.pallas_call(
        functools.partial(exchange_kernel, axis, n, modes),
        out_shape=tuple(jax.ShapeDtypeStruct(shape(a, m), a.dtype) for a, m in zip(arrays, modes)),
        in_specs=[VM] * k,
        out_specs=[VM] * k,
        scratch_shapes=[pltpu.SemaphoreType.DMA((n, k))] * 2,
        compiler_params=params(cid),
        name="exchange",
    )(*arrays)


def flip(z, offset):
    other, bit = z, 1
    while bit <= offset:
        if offset & bit:
            other = other + bit - 2 * bit * lax.rem(z // bit, 2)
        bit *= 2
    return other


def layer_kernel(n_sp, n_tp, groups, capacity, order, *refs):
    f32, bf16 = jnp.float32, jnp.bfloat16
    pieces, refs = refs[:6], refs[6:]
    (stop_a, stop_b, routes_ref, gates_ref, mix_gain, ffn_gain), refs = refs[:6], refs[6:]
    large, refs = refs[:9], refs[9:]
    result_ref, refs = refs[0], refs[1:]
    full, refs = refs[:7], refs[7:]
    made, refs = refs[:2], refs[2:]
    attended, refs = refs[:2], refs[2:]
    held, refs = refs[:9], refs[9:]
    (stops_own, partial, part_out, part_in, aux, stats_out, stats_in, normed_ref), refs = (
        refs[:8],
        refs[8:],
    )
    (out_ref, arrived, returned, made_back, pre, pre_in, hid, s_pre, s_pre_in, s_hid), refs = (
        refs[:10],
        refs[10:],
    )
    (gather_ref, scatter_ref), refs = refs[:2], refs[2:]
    (load_sem, fsend, frecv, rsend, rrecv, osend, orecv, xsend, xrecv, tsend, trecv), refs = (
        refs[:11],
        refs[11:],
    )
    dsend, drecv, bsend, brecv, psend, precv, hsend, hrecv = refs

    me, col = lax.axis_index("sp"), lax.axis_index("tp")
    nz = n_sp // 2
    z, c = me // 2, lax.rem(me, 2)
    partner = z * 2 + 1 - c
    rows = pieces[0].shape[0]
    tall_rows = rows // LANES * LANES + (LANES if rows % LANES else 0)
    w_out_a, w_out_b, resid_ref, w_gate, w_up, w_down, sg_ref, su_ref, sd_ref = held
    experts = w_gate.shape[0]
    width = resid_ref.shape[1]
    block = arrived.shape[1]
    part = hid.shape[2] // n_tp

    def dot(a, b):
        return jnp.dot(a, b, preferred_element_type=f32)

    loads = [pltpu.make_async_copy(a, b, load_sem.at[i]) for i, (a, b) in enumerate(zip(large, held))]
    stops_own[...] = jnp.zeros_like(stops_own)
    heads_a, heads_b = stop_a.shape[0], stop_b.shape[0]
    stops_own[:heads_a, :rows] = stop_a[...]
    stops_own[heads_a : heads_a + heads_b, :rows] = stop_b[...]
    barrier = pltpu.get_barrier_semaphore()
    for d in range(1, n_sp):
        pl.semaphore_signal(
            barrier, inc=1, device_id={"sp": lax.rem(me + d, n_sp)}, device_id_type=MESH
        )
    for d in range(1, n_tp):
        pl.semaphore_signal(
            barrier, inc=1, device_id={"tp": lax.rem(col + d, n_tp)}, device_id_type=MESH
        )
    pl.semaphore_wait(barrier, n_sp + n_tp - 2)

    sends = []

    def remote(source, target, send, recv, where):
        copy = pltpu.make_async_remote_copy(
            src_ref=source,
            dst_ref=target,
            send_sem=send,
            recv_sem=recv,
            device_id=where,
            device_id_type=MESH,
        )
        copy.start()
        sends.append(copy)
        return copy

    def landed(ref, sem):
        pltpu.make_async_copy(ref, ref, sem).wait()

    ins = tuple(pieces) + (stops_own,)
    names = ((6, 0, 1, 2), (3, 4, 5))

    def piece(t, place):
        if t == 6:
            return ins[t]
        return ins[t].at[:, pl.ds(pl.multiple_of(place * LANES, LANES), LANES)]

    def spot(t, source):
        tall = ins[t].shape[0]
        return full[t].at[pl.ds(pl.multiple_of(source * tall, tall), tall), :]

    places = [flip(z, o) for o in range(nz)]
    pushed = {}

    def push(g):
        for t in names[g]:
            for o in range(1, nz):
                pushed[t, o] = remote(
                    piece(t, places[o]),
                    spot(t, me),
                    fsend.at[o, t],
                    frecv.at[z, t],
                    {"sp": places[o] * 2 + c},
                )
            pltpu.make_async_copy(piece(t, z), spot(t, me), frecv.at[z, t]).start()

    push(0)
    for load in loads:
        load.start()

    def relay(g, chip):
        for t in names[g]:
            mine = spot(t, chip * 2 + c)
            landed(mine, frecv.at[chip, t])
            remote(mine, mine, rsend.at[chip, t], rrecv.at[chip, t], {"sp": partner})

    def relayed(g, chip):
        for t in names[g]:
            landed(spot(t, chip * 2 + 1 - c), rrecv.at[chip, t])

    slot_rows = []

    def tables():
        total_experts = n_sp * experts
        kinds = lax.broadcasted_iota(jnp.int32, (total_experts, rows), 0)
        hots = [(kinds == routes_ref[t : t + 1, :]).astype(f32) for t in range(routes_ref.shape[0])]
        named = hots[0]
        for hot in hots[1:]:
            named = named + hot
        before = (
            lax.broadcasted_iota(jnp.int32, (rows, rows), 0)
            < lax.broadcasted_iota(jnp.int32, (rows, rows), 1)
        ).astype(bf16)
        earlier = dot(named.astype(bf16), before)
        aux[...] = jnp.zeros_like(aux)
        for t, hot in enumerate(hots):
            rank = jnp.sum(earlier * hot, axis=0, keepdims=True)
            slot = routes_ref[t : t + 1, :].astype(f32) * float(capacity) + rank
            slot_rows.append(slot)
            aux[t : t + 1, :rows] = slot
            aux[len(hots) + t : len(hots) + t + 1, :rows] = gates_ref[t : t + 1, :]
        spread = gather_ref.shape[0]
        tall = spread // experts

        def where_of(index, k):
            place = index + k * capacity
            for e in range(1, experts):
                place = place + jnp.where(index >= e * capacity, tall - capacity, 0)
            return place

        for k in range(2):
            index = lax.broadcasted_iota(jnp.int32, (spread, LANES), 1)
            hit = where_of(index, k) == lax.broadcasted_iota(jnp.int32, (spread, LANES), 0)
            hit = jnp.logical_and(hit, index < block)
            gather_ref[:, k * LANES : (k + 1) * LANES] = hit.astype(f32).astype(bf16)
            index = lax.broadcasted_iota(jnp.int32, (block, spread), 0)
            hit = where_of(index, k) == lax.broadcasted_iota(jnp.int32, (block, spread), 1)
            scatter_ref[k] = hit.astype(f32).astype(bf16)

    tile = 2 * LANES
    upper = (
        lax.broadcasted_iota(jnp.int32, (tile, tile), 0)
        > lax.broadcasted_iota(jnp.int32, (tile, tile), 1)
    ).astype(bf16)
    lane = lax.broadcasted_iota(jnp.int32, (rows, LANES), 1)
    column = lax.broadcasted_iota(jnp.int32, (rows, tile), 1)
    line = lax.broadcasted_iota(jnp.int32, (rows, tile), 0)

    backs = []
    steps = [(g, m) for g in range(2) for m in range(nz)]
    offsets = (0, heads_a)
    tables()
    for o in range(nz):
        if o == nz - 1:
            push(1)
        relay(0, places[o])
    for number, (g, m) in enumerate(steps):
        relayed(g, m)
        size = groups[g][1]
        heads = LANES // size
        q_ref, k_ref, v_ref = full[3 * g : 3 * g + 3]
        scale = LOG2E * size ** (-0.5)
        block_q = 2 * m + (c if m % 2 == 0 else 1 - c)
        count = -(-(2 * m + 2) * rows // tile)
        query = q_ref[pl.ds(pl.multiple_of(block_q * rows, rows), rows), :]
        lines = stops_own.shape[0]
        stop_t = full[6][pl.ds(pl.multiple_of(block_q * lines, lines), lines), :]
        fill = jnp.zeros((LANES - lines, stop_t.shape[1]), f32)
        stop_all = jnp.concatenate([stop_t, fill], axis=0).T[:rows]
        parts = []
        for h in range(heads):
            head = offsets[g] + z * heads + h
            stop = jnp.sum(jnp.where(lane == head, stop_all, 0.0), axis=1, keepdims=True) * LOG2E
            mine = query * ((lane // size) == h).astype(bf16) if heads > 1 else query
            carry = jnp.zeros((rows, 1), f32)
            total = jnp.zeros((rows, LANES), f32)
            for i in range(count):
                if (g, m, h, i) == (0, nz - 1, heads - 1, count // 2):
                    for o in range(nz):
                        relay(1, places[o])
                begin = block_q * rows + rows - tile * (i + 1)
                short = (2 * m + 1) * rows - tile * (i + 1) < 0
                short = short or (2 * m + 2) * rows - tile * (i + 1) < 0
                masked = i == 0 or short
                start = pl.multiple_of(jnp.maximum(begin, 0), math.gcd(rows, tile))
                keys = k_ref[pl.ds(start, tile), :]
                values = v_ref[pl.ds(start, tile), :]
                score = lax.dot_general(
                    mine, keys, (((1,), (1,)), ((), ())), preferred_element_type=f32
                )
                score = score * scale + stop
                fail = jnp.log2(1.0 + jnp.exp2(jnp.minimum(score, 100.0)))
                fail = jnp.maximum(fail, score)
                hit = score - fail
                if masked:
                    valid = column < begin + tile - start
                    if i == 0:
                        valid = column + start < line + block_q * rows
                    fail = jnp.where(valid, fail, 0.0)
                after = dot(fail.astype(bf16), upper)
                weight = jnp.exp2(hit - after - carry)
                if masked:
                    weight = jnp.where(valid, weight, 0.0)
                carry = carry + after[:, :1] + fail[:, :1]
                total = total + dot(weight.astype(bf16), values)
            parts.append(total)
        merged = parts[0]
        for h in range(1, heads):
            merged = jnp.where(lane // size >= h, parts[h], merged)
        made[g][m] = merged.astype(bf16)
        place = attended[g].at[:, pl.ds(pl.multiple_of(z * LANES, LANES), LANES)]
        backs.append((g, m, block_q))

        @pl.when(block_q != me)
        def _(g=g, m=m, place=place, block_q=block_q):
            pltpu.make_async_remote_copy(
                src_ref=made[g].at[m],
                dst_ref=place,
                send_sem=osend.at[g, m],
                recv_sem=orecv.at[g, z],
                device_id={"sp": block_q},
                device_id_type=MESH,
            ).start()

        @pl.when(block_q == me)
        def _(g=g, m=m, place=place):
            pltpu.make_async_copy(made[g].at[m], place, orecv.at[g, z]).start()


    loads[0].wait()
    loads[1].wait()
    loads[2].wait()

    def columns(which, wide):
        return pl.ds(pl.multiple_of(which * wide, wide), wide)

    peers = [lax.rem(col + d, n_tp) for d in range(1, n_tp)] + [col]
    for g, weights in enumerate((w_out_a, w_out_b)):
        for u in range(groups[g][0]):
            landed(attended[g].at[:, u * LANES : (u + 1) * LANES], orecv.at[g, u])
        left = attended[g][...]
        for i, peer in enumerate(peers):
            term = dot(left, weights[:, columns(peer, width)])
            if g == 0:
                partial[i] = term
                continue
            part_out[i] = (partial[i] + term).astype(bf16)
            if i < n_tp - 1:
                remote(part_out.at[i], part_in.at[i], xsend.at[i], xrecv.at[i], {"tp": peer})
    resid = resid_ref[...].astype(f32)
    mixed = part_out[n_tp - 1].astype(f32)
    for i in range(n_tp - 1):
        landed(part_in.at[i], xrecv.at[i])
        mixed = mixed + part_in[i].astype(f32)

    shaped = mixed * mix_gain[...]
    sums = jnp.zeros((rows, LANES), f32)
    for i, term in enumerate((mixed * mixed, resid * resid, resid * shaped, shaped * shaped)):
        sums = jnp.where(lane == i, jnp.sum(term, axis=1, keepdims=True), sums)
    if tall_rows > rows:
        sums = jnp.concatenate([sums, jnp.zeros((tall_rows - rows, LANES), f32)], axis=0)
    stats_out[...] = sums.T[:8]
    for d in range(1, n_tp):
        remote(
            stats_out, stats_in.at[d - 1], tsend.at[d - 1], trecv.at[d - 1], {"tp": peers[d - 1]}
        )
    sums = stats_out[...]
    for d in range(1, n_tp):
        landed(stats_in.at[d - 1], trecv.at[d - 1])
        sums = sums + stats_in[d - 1]
    sums = jnp.concatenate([sums, jnp.zeros((LANES - 8, tall_rows), f32)], axis=0).T[:rows]
    model = width * n_tp
    scale = lax.rsqrt(sums[:, 0:1] / model + epsilon)
    stream = (resid + shaped * scale).astype(bf16)
    square = sums[:, 1:2] + scale * (2.0 * sums[:, 2:3] + scale * sums[:, 3:4])
    square = jnp.maximum(square, 0.0)
    stream = stream.astype(f32)
    result_ref[...] = stream
    normed = stream * lax.rsqrt(square / model + epsilon) * ffn_gain[...]
    normed_ref[...] = normed.astype(bf16)

    chips = [flip(z, o) for o in order]
    shared = len(chips)
    seat = lax.broadcasted_iota(jnp.int32, (block, rows), 0)
    for i, o in enumerate(order):
        for k in range(2):
            peer = chips[i] * 2 + lax.rem(c + k, 2)
            seats = (seat + peer * block).astype(f32)
            chosen = seats == slot_rows[0]
            for slot in slot_rows[1:]:
                chosen = jnp.logical_or(chosen, seats == slot)
            picked = dot(chosen.astype(f32).astype(bf16), normed_ref[...])
            out_ref[2 * i + k] = picked.astype(bf16)
            if o == 0 and k == 0:
                pltpu.make_async_copy(out_ref.at[2 * i + k], arrived.at[me], drecv.at[me]).start()
            else:
                remote(
                    out_ref.at[2 * i + k],
                    arrived.at[me],
                    dsend.at[2 * i + k],
                    drecv.at[me],
                    {"sp": peer},
                )

    def buffers(i):
        if i == shared:
            return s_pre, s_pre_in, s_hid
        return pre.at[i], pre_in.at[i], hid.at[i]

    def first(i):
        here, there, _ = buffers(i)
        if i == shared:
            loads[6].wait()
            loads[7].wait()
            for k, weight in enumerate((sg_ref, su_ref)):
                here[k] = dot(normed_ref[...], weight[...]).astype(bf16)
        else:
            grouped = None
            for k in range(2):
                source = chips[i] * 2 + k
                landed(arrived.at[source], drecv.at[source])
                term = dot(gather_ref[:, k * LANES : k * LANES + block], arrived[source])
                grouped = term if grouped is None else grouped + term
            grouped = grouped.astype(bf16)
            tall = grouped.shape[0] // experts
            if i == 0:
                loads[3].wait()
                loads[4].wait()
            for k, weight in enumerate((w_gate, w_up)):
                terms = [
                    dot(grouped[e * tall : (e + 1) * tall], weight[e]).astype(bf16)
                    for e in range(experts)
                ]
                spread_rows = jnp.concatenate(terms, axis=0)
                here[k] = jnp.concatenate(
                    [dot(scatter_ref[j], spread_rows) for j in range(2)], axis=0
                ).astype(bf16)
        for d in range(1, n_tp):
            for k in range(2):
                remote(
                    here.at[k, :, columns(peers[d - 1], part)],
                    there.at[d - 1, k],
                    psend.at[i, d - 1, k],
                    precv.at[i, d - 1, k],
                    {"tp": peers[d - 1]},
                )

    def second(i):
        here, there, whole = buffers(i)
        sums = []
        for k in range(2):
            total = here[k, :, columns(col, part)].astype(f32)
            for d in range(1, n_tp):
                landed(there.at[d - 1, k], precv.at[i, d - 1, k])
                total = total + there[d - 1, k].astype(f32)
            sums.append(total)
        whole[:, columns(col, part)] = (sums[0] / (1.0 + jnp.exp(-sums[0])) * sums[1]).astype(bf16)
        for d in range(1, n_tp):
            mine = whole.at[:, columns(col, part)]
            remote(mine, mine, hsend.at[i, d - 1], hrecv.at[i, d - 1], {"tp": peers[d - 1]})

    kept = []

    def third(i):
        _, _, whole = buffers(i)
        for d in range(1, n_tp):
            source = lax.rem(col + n_tp - d, n_tp)
            landed(whole.at[:, columns(source, part)], hrecv.at[i, d - 1])
        if i == shared:
            loads[8].wait()
            result_ref[...] = result_ref[...] + dot(whole[...], sd_ref[...])
            return
        hidden = whole[...]
        grouped = dot(gather_ref[:, :block], hidden[:block]) + dot(
            gather_ref[:, LANES : LANES + block], hidden[block:]
        )
        grouped = grouped.astype(bf16)
        tall = grouped.shape[0] // experts
        if i == 0:
            loads[5].wait()
        terms = [
            dot(grouped[e * tall : (e + 1) * tall], w_down[e]).astype(bf16) for e in range(experts)
        ]
        terms = jnp.concatenate(terms, axis=0)
        for k in range(2):
            source = chips[i] * 2 + k
            made_back[i, k] = dot(scatter_ref[k], terms).astype(bf16)
            if order[i] == 0:

                @pl.when(source != me)
                def _():
                    pltpu.make_async_remote_copy(
                        src_ref=made_back.at[i, k],
                        dst_ref=returned.at[me],
                        send_sem=bsend.at[i, k],
                        recv_sem=brecv.at[me],
                        device_id={"sp": source},
                        device_id_type=MESH,
                    ).start()

                @pl.when(source == me)
                def _():
                    pltpu.make_async_copy(made_back.at[i, k], returned.at[me], brecv.at[me]).start()

                kept.append((i, k, source))
            else:
                remote(
                    made_back.at[i, k],
                    returned.at[me],
                    bsend.at[i, k],
                    brecv.at[me],
                    {"sp": source},
                )

    top_count = routes_ref.shape[0]
    turned = aux[...].T[:rows]
    taken = lax.broadcasted_iota(jnp.int32, (rows, block), 1)

    def combine(i):
        total = result_ref[...]
        for k in range(2):
            source = chips[i] * 2 + k
            landed(returned.at[source], brecv.at[source])
            seats = (taken + source * block).astype(f32)
            gated = jnp.zeros(seats.shape, f32)
            for t in range(top_count):
                gate = turned[:, top_count + t : top_count + t + 1]
                gated = gated + jnp.where(seats == turned[:, t : t + 1], gate, 0.0)
            high = gated.astype(bf16)
            low = (gated - high.astype(f32)).astype(bf16)
            total = total + dot(high, returned[source]) + dot(low, returned[source])
        result_ref[...] = total

    first(shared)
    first(0)
    second(shared)
    for i in range(1, shared + 2):
        if i < shared:
            first(i)
        if i <= shared:
            second(i - 1)
        if i == 1:
            third(shared)
        else:
            third(i - 2)
        if i >= 4:
            combine(i - 4)
    for i in range(max(shared - 2, 0), shared):
        combine(i)
    for copy in sends:
        copy.wait_send()
    for g, m, block_q in backs:

        @pl.when(block_q != me)
        def _(g=g, m=m):
            landed(made[g].at[m], osend.at[g, m])

    for i, k, source in kept:

        @pl.when(source != me)
        def _(i=i, k=k):
            landed(made_back.at[i, k], bsend.at[i, k])


def layer(n_sp, n_tp, groups, capacity, arrays, small, large):
    f32, bf16 = jnp.float32, jnp.bfloat16
    rows = arrays[0].shape[0]
    resid, w_gate = large[2], large[3]
    width = resid.shape[1]
    experts, hidden_width = w_gate.shape[0], w_gate.shape[2]
    block = experts * capacity
    nz = n_sp // 2
    order = tuple(range(nz // 2, nz)) + tuple(range(nz // 2 - 1, -1, -1))
    wide = -(-rows // LANES) * LANES
    lines = -(-(small[0].shape[0] + small[1].shape[0]) // 8) * 8
    tall = -(-2 * capacity // 16) * 16
    part = hidden_width // n_tp
    dma = pltpu.SemaphoreType.DMA
    vmem = pltpu.VMEM
    anywhere = pl.BlockSpec(memory_space=pl.ANY)
    scratch = (
        [vmem((n_sp * rows, LANES), bf16)] * 6
        + [vmem((n_sp * lines, wide), f32)]
        + [vmem((nz, rows, LANES), bf16)] * 2
        + [vmem((rows, units * LANES), bf16) for units, _ in groups]
        + [vmem(a.shape, a.dtype) for a in large]
        + [
            vmem((lines, wide), f32),
            vmem((n_tp, rows, width), f32),
            vmem((n_tp, rows, width), bf16),
            vmem((n_tp - 1, rows, width), bf16),
            vmem((LANES, wide), f32),
            vmem((8, wide), f32),
            vmem((n_tp - 1, 8, wide), f32),
            vmem((rows, width), bf16),
        ]
        + [
            vmem((n_sp, block, width), bf16),
            vmem((n_sp, block, width), bf16),
            vmem((n_sp, block, width), bf16),
            vmem((nz, 2, block, width), bf16),
            vmem((nz, 2, 2 * block, hidden_width), bf16),
            vmem((nz, n_tp - 1, 2, 2 * block, part), bf16),
            vmem((nz, 2 * block, hidden_width), bf16),
            vmem((2, rows, hidden_width), bf16),
            vmem((n_tp - 1, 2, rows, part), bf16),
            vmem((rows, hidden_width), bf16),
        ]
        + [vmem((experts * tall, 2 * LANES), bf16), vmem((2, block, experts * tall), bf16)]
        + [dma((len(large),))]
        + [dma((nz, 7))] * 4
        + [dma((2, nz))] * 2
        + [dma((n_tp - 1,))] * 4
        + [dma((n_sp,)), dma((n_sp,)), dma((nz, 2)), dma((n_sp,))]
        + [dma((nz + 1, n_tp - 1, 2))] * 2
        + [dma((nz + 1, n_tp - 1))] * 2
    )
    return pl.pallas_call(
        functools.partial(layer_kernel, n_sp, n_tp, groups, capacity, order),
        out_shape=pltpu.VMEM((rows, width), f32),
        in_specs=[VM] * 12 + [anywhere] * 9,
        out_specs=VM,
        scratch_shapes=scratch,
        compiler_params=params(9),
        name="layer",
    )(*arrays, *small, *large)


def shards(
    n_sp,
    n_tp,
    query_a,
    key_a,
    value_a,
    query_b,
    key_b,
    value_b,
    stop_a,
    stop_b,
    out_a,
    out_b,
    resid,
    mix_gain,
    ffn_gain,
    routes,
    gates,
    exp_gate,
    exp_up,
    exp_down,
    sh_gate,
    sh_up,
    sh_down,
):
    f32, bf16 = jnp.float32, jnp.bfloat16
    rows = query_a.shape[0]
    heads_a, heads_b = stop_a.shape[1], stop_b.shape[1]
    units_a, units_b = query_a.shape[1] // LANES, query_b.shape[1] // LANES
    width = resid.shape[1]
    model = width * n_tp

    local_experts = exp_gate.shape[0]
    experts = local_experts * n_sp
    top_count = routes.shape[1]
    capacity = max(1, (3 * rows * top_count + 2 * experts - 1) // (2 * experts))
    block = local_experts * capacity
    hidden_width = exp_gate.shape[2]
    groups = ((units_a, query_a.shape[1] // heads_a), (units_b, query_b.shape[1] // heads_b))
    fused = (
        (hidden_width // n_tp) % LANES == 0
        and width % LANES == 0
        and block % 8 == 0
        and block <= LANES
        and exp_gate.shape == exp_down.shape
        and all(2 * units == n_sp for units, _ in groups)
        and (n_sp // 2) & (n_sp // 2 - 1) == 0
        and 2 * rows <= 4 * LANES
    )
    if fused:
        arrays = (query_a, key_a, value_a, query_b, key_b, value_b)
        small = (stop_a.T, stop_b.T, routes.T, gates.T, mix_gain[None, :], ffn_gain[None, :])
        large = (out_a, out_b, resid, exp_gate, exp_up, exp_down, sh_gate, sh_up, sh_down)
        return layer(n_sp, n_tp, groups, capacity, arrays, small, large).astype(bf16)

    flat_routes = routes.reshape(-1)
    onehot = (flat_routes[:, None] == jnp.arange(experts, dtype=jnp.int32)[None, :]).astype(f32)
    pairs = rows * top_count
    before = (jnp.arange(pairs)[:, None] > jnp.arange(pairs)[None, :]).astype(bf16)
    earlier = jnp.dot(before, onehot.astype(bf16), preferred_element_type=f32)
    slot = flat_routes * capacity + jnp.sum(earlier * onehot, axis=1).astype(jnp.int32)
    slot = slot.reshape(rows, top_count)
    slots = jnp.arange(experts * capacity, dtype=jnp.int32)
    chosen = slot[:, :, None] == slots[None, None, :]
    chooser = jnp.sum(chosen.astype(f32), axis=1).astype(bf16)
    gated = jnp.sum(jnp.where(chosen, gates[:, :, None], 0.0), axis=1)
    gated_high = gated.astype(bf16)
    gated_low = (gated - gated_high.astype(f32)).astype(bf16)

    stops = jnp.concatenate([stop_a, stop_b], axis=1)
    lines = -(-stops.shape[1] // 8) * 8
    wide = -(-rows // LANES) * LANES
    stops = jnp.pad(stops.T, ((0, lines - stops.shape[1]), (0, wide - rows)))
    arrays = (query_a, key_a, value_a, query_b, key_b, value_b, stops)
    attended_a, attended_b = stick(n_sp, rows, arrays, groups, (0, heads_a), 0)

    partial_value = jnp.dot(attended_a, out_a, preferred_element_type=f32)
    partial_value = partial_value + jnp.dot(attended_b, out_b, preferred_element_type=f32)
    (pieces,) = exchange("tp", n_tp, (partial_value.astype(bf16),), ("cols",), 2)
    mixed = jnp.sum(pieces.astype(f32), axis=0)
    resid_f = resid.astype(f32)
    shaped = mixed * mix_gain[None, :]
    sums = jnp.stack(
        [
            jnp.sum(mixed * mixed, axis=1),
            jnp.sum(resid_f * resid_f, axis=1),
            jnp.sum(resid_f * shaped, axis=1),
            jnp.sum(shaped * shaped, axis=1),
        ]
    )
    sums = jnp.pad(sums, ((0, 4), (0, wide - rows)))
    (sums,) = exchange("tp", n_tp, (sums,), ("all",), 3)
    sums = jnp.sum(sums, axis=0)[:4, :rows]
    scale = lax.rsqrt(sums[0] / model + epsilon)
    stream = (resid_f + shaped * scale[:, None]).astype(bf16)
    square = jnp.maximum(sums[1] + scale * (2.0 * sums[2] + scale * sums[3]), 0.0)
    stream_f = stream.astype(f32)
    normed = (stream_f * lax.rsqrt(square / model + epsilon)[:, None] * ffn_gain[None, :]).astype(bf16)

    outgoing = lax.dot_general(chooser, normed, (((0,), (0,)), ((), ())), preferred_element_type=f32)
    outgoing = outgoing.astype(bf16).reshape(n_sp, local_experts * capacity, width)
    (arrived,) = exchange("sp", n_sp, (outgoing,), ("lead",), 4)
    arrived = arrived.reshape(n_sp, local_experts, capacity, width)
    arrived = jnp.transpose(arrived, (1, 0, 2, 3)).reshape(local_experts, n_sp * capacity, width)

    shared_parts = [
        jnp.dot(normed, w, preferred_element_type=f32).astype(bf16) for w in (sh_gate, sh_up)
    ]
    expert_parts = [
        jnp.einsum("erd,edf->erf", arrived, w, preferred_element_type=f32)
        .astype(bf16)
        .reshape(local_experts * n_sp * capacity, -1)
        for w in (exp_gate, exp_up)
    ]
    parts = exchange("tp", n_tp, (*expert_parts, *shared_parts), ("cols",) * 4, 5)
    gate_pre, up_pre, shared_gate, shared_up = [jnp.sum(p.astype(f32), axis=0) for p in parts]
    hidden = (jax.nn.silu(gate_pre) * up_pre).astype(bf16)
    shared_hidden = (jax.nn.silu(shared_gate) * shared_up).astype(bf16)
    hidden, shared_hidden = exchange("tp", n_tp, (hidden, shared_hidden), ("side",) * 2, 6)

    shared_out = jnp.dot(shared_hidden, sh_down, preferred_element_type=f32)
    hidden = hidden.reshape(local_experts, n_sp * capacity, -1)
    produced = jnp.einsum("erf,efd->erd", hidden, exp_down, preferred_element_type=f32).astype(bf16)
    produced = produced.reshape(local_experts, n_sp, capacity, width)
    produced = jnp.transpose(produced, (1, 0, 2, 3)).reshape(n_sp, local_experts * capacity, width)
    (returned,) = exchange("sp", n_sp, (produced,), ("lead",), 7)
    flat_back = returned.reshape(experts * capacity, width)
    routed = jnp.dot(gated_high, flat_back, preferred_element_type=f32)
    routed = routed + jnp.dot(gated_low, flat_back, preferred_element_type=f32)
    moe = routed + shared_out
    return (stream_f + moe).astype(bf16)


def solution(mesh):
    return jax.shard_map(
        functools.partial(shards, mesh.shape["sp"], mesh.shape["tp"]),
        mesh=mesh,
        in_specs=(
            P("sp", "tp"),
            P("sp", "tp"),
            P("sp", "tp"),
            P("sp", "tp"),
            P("sp", "tp"),
            P("sp", "tp"),
            P("sp", "tp"),
            P("sp", "tp"),
            P("tp", None),
            P("tp", None),
            P("sp", "tp"),
            P("tp"),
            P("tp"),
            P("sp", None),
            P("sp", None),
            P("sp", "tp", None),
            P("sp", "tp", None),
            P("sp", None, "tp"),
            P("tp", None),
            P("tp", None),
            P(None, "tp"),
        ),
        out_specs=P("sp", "tp"),
        check_vma=False,
    )
```

```python
import functools
import math

import jax
import jax.numpy as jnp
import numpy as np
from jax import lax
from jax.experimental import pallas as pl
from jax.experimental.pallas import tpu as pltpu
from jax.sharding import PartitionSpec as P

MESH = pl.DeviceIdType.MESH
LANES = 128
LOG2E = 1.4426950408889634
epsilon = 1e-06
VM = pl.BlockSpec(memory_space=pltpu.VMEM)


def greet(axis, peers):
    barrier = pltpu.get_barrier_semaphore()
    for peer in peers:
        pl.semaphore_signal(barrier, inc=1, device_id={axis: peer}, device_id_type=MESH)
    pl.semaphore_wait(barrier, len(peers))


def params(cid):
    return pltpu.CompilerParams(
        collective_id=cid, has_side_effects=True, vmem_limit_bytes=56 * 1024 * 1024
    )


def snake(r, j, m):
    return m * r + (j if m % 2 == 0 else r - 1 - j)


def stick_kernel(n, rows, groups, offsets, *refs):
    g_count = len(groups)
    count = 3 * g_count + 1
    ins, outs = refs[:count], refs[count : count + g_count]
    full = refs[count + g_count : 2 * count + g_count]
    made = refs[2 * count + g_count : 2 * count + 2 * g_count]
    send, recv, rsend, rrecv, own, bsend, brecv = refs[2 * count + 2 * g_count :]
    me = lax.axis_index("sp")
    nz = n // 2
    z, c = me // 2, lax.rem(me, 2)
    partner = z * 2 + 1 - c
    places = [lax.rem(z + d, nz) for d in range(nz)]
    greet("sp", [lax.rem(me + d, n) for d in range(1, n)])
    order = [count - 1] + list(range(count - 1))

    def piece(t, place):
        if t == count - 1:
            return ins[t]
        unit = (2 * place) // (n // groups[t // 3][0])
        return ins[t].at[:, pl.ds(pl.multiple_of(unit * LANES, LANES), LANES)]

    def spot(t, source):
        tall = ins[t].shape[0]
        return full[t].at[pl.ds(pl.multiple_of(source * tall, tall), tall), :]

    def remote(source, target, send_sem, recv_sem, device):
        copy = pltpu.make_async_remote_copy(
            src_ref=source,
            dst_ref=target,
            send_sem=send_sem,
            recv_sem=recv_sem,
            device_id={"sp": device},
            device_id_type=MESH,
        )
        copy.start()
        return copy

    first, relays, local = {}, {}, {}
    for t in order:
        for d in range(1, nz):
            first[d, t] = remote(
                piece(t, places[d]), spot(t, me), send.at[d, t], recv.at[d, t], places[d] * 2 + c
            )
        relays[0, t] = remote(piece(t, z), spot(t, me), rsend.at[0, t], rrecv.at[0, t], partner)
        local[t] = pltpu.make_async_copy(piece(t, z), spot(t, me), own.at[t])
        local[t].start()

    def relay(d, t):
        source = lax.rem(z + nz - d, nz) * 2 + c
        first[d, t].wait_recv()
        relays[d, t] = remote(
            spot(t, source), spot(t, source), rsend.at[d, t], rrecv.at[d, t], partner
        )

    def arrive(t):
        local[t].wait()
        for d in range(nz):
            relays[d, t].wait_recv()

    group_arrays = lambda g: ([count - 1] if g == 0 else []) + [3 * g, 3 * g + 1, 3 * g + 2]
    for d in range(1, nz):
        for t in group_arrays(0):
            relay(d, t)

    tile = 2 * LANES
    upper = (
        lax.broadcasted_iota(jnp.int32, (tile, tile), 0)
        > lax.broadcasted_iota(jnp.int32, (tile, tile), 1)
    ).astype(jnp.bfloat16)
    lane = lax.broadcasted_iota(jnp.int32, (rows, LANES), 1)
    column = lax.broadcasted_iota(jnp.int32, (rows, tile), 1)
    line = lax.broadcasted_iota(jnp.int32, (rows, tile), 0)
    backs = []
    for g in range(g_count):
        units, size = groups[g]
        q_ref, k_ref, v_ref = full[3 * g : 3 * g + 3]
        r = n // units
        unit, j = me // r, lax.rem(me, r)
        heads = LANES // size
        scale = LOG2E * size ** (-0.5)
        for t in group_arrays(g):
            arrive(t)
        pending = []
        if g + 1 < g_count:
            pending = [(d, t) for d in range(1, nz) for t in group_arrays(g + 1)]
        for m in range(n // r):
            block = snake(r, j, m)
            last = lambda b: ((b + 1) * rows - 1) // tile
            counts = [last(snake(r, jj, m)) + 1 for jj in range(r)]
            query = q_ref[pl.ds(pl.multiple_of(block * rows, rows), rows), :]
            lines = ins[count - 1].shape[0]
            stop_t = full[count - 1][pl.ds(pl.multiple_of(block * lines, lines), lines), :]
            fill = jnp.zeros((LANES - lines, stop_t.shape[1]), jnp.float32)
            stop_all = jnp.concatenate([stop_t, fill], axis=0).T[:rows]
            parts = []
            for h in range(heads):
                head = offsets[g] + unit * heads + h
                stop = jnp.sum(jnp.where(lane == head, stop_all, 0.0), axis=1, keepdims=True) * LOG2E
                if heads > 1:
                    mine = query * ((lane // size) == h).astype(jnp.bfloat16)
                else:
                    mine = query
                carry = jnp.zeros((rows, 1), jnp.float32)
                total = jnp.zeros((rows, LANES), jnp.float32)
                for i in range(max(counts)):
                    where_tile = (block * rows + rows - 1) // tile - i
                    masked = i < 2 or i >= min(counts)
                    start = pl.multiple_of(jnp.maximum(where_tile, 0) * tile, tile)
                    keys = k_ref[pl.ds(start, tile), :]
                    values = v_ref[pl.ds(start, tile), :]
                    score = lax.dot_general(
                        mine, keys, (((1,), (1,)), ((), ())), preferred_element_type=jnp.float32
                    )
                    score = score * scale + stop
                    small = jnp.log2(1.0 + jnp.exp2(-jnp.abs(score)))
                    fail = jnp.maximum(score, 0.0) + small
                    hit = score - fail
                    if masked:
                        valid = column + where_tile * tile < line + block * rows
                        if i >= min(counts):
                            valid = jnp.logical_and(valid, where_tile >= 0)
                        fail = jnp.where(valid, fail, 0.0)
                    high = fail.astype(jnp.bfloat16)
                    low = (fail - high.astype(jnp.float32)).astype(jnp.bfloat16)
                    after = jnp.dot(high, upper, preferred_element_type=jnp.float32) + jnp.dot(
                        low, upper, preferred_element_type=jnp.float32
                    )
                    weight = jnp.exp2(hit - after - carry)
                    if masked:
                        weight = jnp.where(valid, weight, 0.0)
                    carry = carry + after[:, :1] + fail[:, :1]
                    total = total + jnp.dot(
                        weight.astype(jnp.bfloat16), values, preferred_element_type=jnp.float32
                    )
                parts.append(total)
            merged = parts[0]
            for h in range(1, heads):
                merged = jnp.where(lane // size >= h, parts[h], merged)
            made[g][m] = merged.astype(jnp.bfloat16)
            place = outs[g].at[:, pl.ds(pl.multiple_of(unit * LANES, LANES), LANES)]

            @pl.when(block != me)
            def _():
                pltpu.make_async_remote_copy(
                    src_ref=made[g].at[m],
                    dst_ref=place,
                    send_sem=bsend.at[g, m],
                    recv_sem=brecv.at[g, unit],
                    device_id={"sp": block},
                    device_id_type=MESH,
                ).start()

            @pl.when(block == me)
            def _():
                pltpu.make_async_copy(made[g].at[m], place, bsend.at[g, m]).start()

            share = -(-len(pending) // (n // r - m))
            for d, t in pending[:share]:
                relay(d, t)
            pending = pending[share:]

    for g in range(g_count):
        r = n // groups[g][0]
        turn, rest = me // r, lax.rem(me, r)
        owner = jnp.where(lax.rem(turn, 2) == 0, rest, r - 1 - rest)
        for u in range(groups[g][0]):

            @pl.when(u * r + owner != me)
            def _(g=g, u=u):
                place = outs[g].at[:, pl.ds(u * LANES, LANES)]
                pltpu.make_async_copy(place, place, brecv.at[g, u]).wait()

        unit = me // r
        place = outs[g].at[:, pl.ds(pl.multiple_of(unit * LANES, LANES), LANES)]
        for m in range(groups[g][0]):
            pltpu.make_async_copy(made[g].at[m], place, bsend.at[g, m]).wait()
    for copy in first.values():
        copy.wait_send()
    for copy in relays.values():
        copy.wait_send()


def stick(n, rows, arrays, groups, offsets, cid):
    k, g_count = len(arrays), len(groups)
    nz, top = n // 2, max(units for units, _ in groups)
    dma = pltpu.SemaphoreType.DMA
    return pl.pallas_call(
        functools.partial(stick_kernel, n, rows, groups, offsets),
        out_shape=tuple(
            jax.ShapeDtypeStruct((rows, units * LANES), jnp.bfloat16) for units, _ in groups
        ),
        in_specs=[VM] * k,
        out_specs=[VM] * g_count,
        scratch_shapes=[
            pltpu.VMEM((n * a.shape[0], LANES if i < k - 1 else a.shape[1]), a.dtype)
            for i, a in enumerate(arrays)
        ]
        + [pltpu.VMEM((units, rows, LANES), jnp.bfloat16) for units, _ in groups]
        + [dma((nz, k))] * 4
        + [dma((k,)), dma((g_count, top)), dma((g_count, top))],
        compiler_params=params(cid),
        name="stick",
    )(*arrays)


def exchange_kernel(axis, n, modes, *refs):
    count = len(modes)
    ins, outs = refs[:count], refs[count : 2 * count]
    send, recv = refs[2 * count :]
    me = lax.axis_index(axis)
    greet(axis, [lax.rem(me + d, n) for d in range(1, n)])

    def ends(t, peer):
        if modes[t] == "lead":
            return ins[t].at[peer], outs[t].at[me]
        if modes[t] == "cols":
            width = ins[t].shape[1] // n
            return ins[t].at[:, pl.ds(pl.multiple_of(peer * width, width), width)], outs[t].at[me]
        if modes[t] == "all":
            return ins[t], outs[t].at[me]
        width = ins[t].shape[1]
        return ins[t], outs[t].at[:, pl.ds(pl.multiple_of(me * width, width), width)]

    copies = []
    for d in range(1, n):
        peer = lax.rem(me + d, n)
        for t in range(count):
            source, target = ends(t, peer)
            copies.append(
                pltpu.make_async_remote_copy(
                    src_ref=source,
                    dst_ref=target,
                    send_sem=send.at[d, t],
                    recv_sem=recv.at[d, t],
                    device_id={axis: peer},
                    device_id_type=MESH,
                )
            )
            copies[-1].start()
    for t in range(count):
        source, target = ends(t, me)
        copies.append(pltpu.make_async_copy(source, target, send.at[0, t]))
        copies[-1].start()
    for copy in copies:
        copy.wait()


def exchange(axis, n, arrays, modes, cid):
    def shape(a, mode):
        if mode == "lead":
            return a.shape
        if mode == "cols":
            return (n, a.shape[0], a.shape[1] // n)
        if mode == "all":
            return (n,) + a.shape
        return (a.shape[0], a.shape[1] * n)

    if modes[0] == "cols" and any((a.shape[1] // n) % LANES for a in arrays):
        cut = [jnp.transpose(a.reshape(a.shape[0], n, -1), (1, 0, 2)) for a in arrays]
        return exchange(axis, n, cut, ("lead",) * len(cut), cid)
    if modes[0] == "side" and any(a.shape[1] % LANES for a in arrays):
        stacked = exchange(axis, n, arrays, ("all",) * len(arrays), cid)
        return [jnp.transpose(a, (1, 0, 2)).reshape(a.shape[1], -1) for a in stacked]
    k = len(arrays)
    return pl.pallas_call(
        functools.partial(exchange_kernel, axis, n, modes),
        out_shape=tuple(jax.ShapeDtypeStruct(shape(a, m), a.dtype) for a, m in zip(arrays, modes)),
        in_specs=[VM] * k,
        out_specs=[VM] * k,
        scratch_shapes=[pltpu.SemaphoreType.DMA((n, k))] * 2,
        compiler_params=params(cid),
        name="exchange",
    )(*arrays)


def flip(z, offset):
    other, bit = z, 1
    while bit <= offset:
        if offset & bit:
            other = other + bit - 2 * bit * lax.rem(z // bit, 2)
        bit *= 2
    return other


def layer_kernel(n_sp, n_tp, groups, capacity, order, *refs):
    f32, bf16 = jnp.float32, jnp.bfloat16
    pieces, refs = refs[:6], refs[6:]
    (stop_a, stop_b, routes_ref, gates_ref, mix_gain, ffn_gain), refs = refs[:6], refs[6:]
    large, refs = refs[:9], refs[9:]
    result_ref, refs = refs[0], refs[1:]
    full, refs = refs[:7], refs[7:]
    near, refs = refs[:6], refs[6:]
    home, refs = refs[:4], refs[4:]
    left_refs, refs = refs[:2], refs[2:]
    made, refs = refs[:2], refs[2:]
    attended, refs = refs[:2], refs[2:]
    held, refs = refs[:9], refs[9:]
    (stops_own, partial, part_out, part_in, aux, stats_out, stats_in, normed_ref), refs = (
        refs[:8],
        refs[8:],
    )
    (out_ref, arrived, returned, made_back, pre, pre_in, hid, s_pre, s_pre_in, s_hid), refs = (
        refs[:10],
        refs[10:],
    )
    (gather_ref, scatter_ref), refs = refs[:2], refs[2:]
    (load_sem, fsend, frecv, rsend, rrecv, osend, orecv, xsend, xrecv, tsend, trecv), refs = (
        refs[:11],
        refs[11:],
    )
    dsend, drecv, bsend, brecv, psend, precv, hsend, hrecv, nsend, nrecv = refs

    me, col = lax.axis_index("sp"), lax.axis_index("tp")
    nz = n_sp // 2
    z, c = me // 2, lax.rem(me, 2)
    partner = z * 2 + 1 - c
    rows = pieces[0].shape[0]
    own = pl.ds(pl.multiple_of(c * rows, rows), rows)
    tall_rows = rows // LANES * LANES + (LANES if rows % LANES else 0)
    w_out_a, w_out_b, resid_ref, w_gate, w_up, w_down, sg_ref, su_ref, sd_ref = held
    experts = w_gate.shape[0]
    width = resid_ref.shape[1]
    block = arrived.shape[1]
    part = hid.shape[2] // n_tp

    def dot(a, b):
        return jnp.dot(a, b, preferred_element_type=f32)

    taken_in = [
        pltpu.make_async_copy(
            a, near[t] if t % 3 == 0 else near[t].at[own, :], load_sem.at[len(large) + t]
        )
        for t, a in enumerate(pieces)
    ]
    for copy in taken_in:
        copy.start()
    loads = [pltpu.make_async_copy(a, b, load_sem.at[i]) for i, (a, b) in enumerate(zip(large, held))]
    stops_own[...] = jnp.zeros_like(stops_own)
    heads_a, heads_b = stop_a.shape[0], stop_b.shape[0]
    stops_own[:heads_a, :rows] = stop_a[...]
    stops_own[heads_a : heads_a + heads_b, :rows] = stop_b[...]
    barrier = pltpu.get_barrier_semaphore()
    for d in range(1, n_sp):
        pl.semaphore_signal(
            barrier, inc=1, device_id={"sp": lax.rem(me + d, n_sp)}, device_id_type=MESH
        )
    for d in range(1, n_tp):
        pl.semaphore_signal(
            barrier, inc=1, device_id={"tp": lax.rem(col + d, n_tp)}, device_id_type=MESH
        )
    pl.semaphore_wait(barrier, n_sp + n_tp - 2)

    sends = []

    def remote(source, target, send, recv, where):
        copy = pltpu.make_async_remote_copy(
            src_ref=source,
            dst_ref=target,
            send_sem=send,
            recv_sem=recv,
            device_id=where,
            device_id_type=MESH,
        )
        copy.start()
        sends.append(copy)
        return copy

    def landed(ref, sem):
        pltpu.make_async_copy(ref, ref, sem).wait()

    ends = nz - 1
    names = ((6, 0), (1, 2)), ((3,), (4, 5))

    def piece(t, place):
        if t == 6:
            return stops_own
        lanes = pl.ds(pl.multiple_of(place * LANES, LANES), LANES)
        return near[t].at[:, lanes] if t % 3 == 0 else near[t].at[own, lanes]

    def spot(t, source):
        tall = stops_own.shape[0] if t == 6 else rows
        return full[t].at[pl.ds(pl.multiple_of(source * tall, tall), tall), :]

    places = [flip(z, o) for o in range(nz)]

    def push(g):
        for part_names, needed in ((names[g][1], z < ends), (names[g][0], z > 0)):

            @pl.when(needed)
            def _(part_names=part_names):
                for t in part_names:
                    for o in range(1, nz):
                        pltpu.make_async_remote_copy(
                            src_ref=piece(t, places[o]),
                            dst_ref=spot(t, me),
                            send_sem=fsend.at[o, t],
                            recv_sem=frecv.at[z, t],
                            device_id={"sp": places[o] * 2 + c},
                            device_id_type=MESH,
                        ).start()
                    pltpu.make_async_copy(piece(t, z), spot(t, me), frecv.at[z, t]).start()

    def pushed(g):
        for part_names, needed in ((names[g][1], z < ends), (names[g][0], z > 0)):

            @pl.when(needed)
            def _(part_names=part_names):
                for t in part_names:
                    for o in range(1, nz):
                        landed(piece(t, places[o]), fsend.at[o, t])

    for copy in taken_in:
        copy.wait()
    for t in (1, 2, 4, 5):
        mine = near[t].at[own, :]
        remote(mine, mine, nsend.at[t], nrecv.at[t], {"sp": partner})
    push(0)
    for load in loads:
        load.start()

    def relay(g, chip):
        for t in names[g][1]:
            mine = spot(t, chip * 2 + c)
            landed(mine, frecv.at[chip, t])
            remote(mine, mine, rsend.at[chip, t], rrecv.at[chip, t], {"sp": partner})

    def relayed(g, chip):
        for t in names[g][1]:
            landed(spot(t, chip * 2 + 1 - c), rrecv.at[chip, t])

    slot_rows = []

    def tables():
        total_experts = n_sp * experts
        kinds = lax.broadcasted_iota(jnp.int32, (total_experts, rows), 0)
        hots = [(kinds == routes_ref[t : t + 1, :]).astype(f32) for t in range(routes_ref.shape[0])]
        named = hots[0]
        for hot in hots[1:]:
            named = named + hot
        before = (
            lax.broadcasted_iota(jnp.int32, (rows, rows), 0)
            < lax.broadcasted_iota(jnp.int32, (rows, rows), 1)
        ).astype(bf16)
        earlier = dot(named.astype(bf16), before)
        aux[...] = jnp.zeros_like(aux)
        for t, hot in enumerate(hots):
            rank = jnp.sum(earlier * hot, axis=0, keepdims=True)
            slot = routes_ref[t : t + 1, :].astype(f32) * float(capacity) + rank
            slot_rows.append(slot)
            aux[t : t + 1, :rows] = slot
            aux[len(hots) + t : len(hots) + t + 1, :rows] = gates_ref[t : t + 1, :]
        spread = gather_ref.shape[0]
        tall = spread // experts

        def where_of(index, k):
            place = index + k * capacity
            for e in range(1, experts):
                place = place + jnp.where(index >= e * capacity, tall - capacity, 0)
            return place

        for k in range(2):
            index = lax.broadcasted_iota(jnp.int32, (spread, LANES), 1)
            hit = where_of(index, k) == lax.broadcasted_iota(jnp.int32, (spread, LANES), 0)
            hit = jnp.logical_and(hit, index < block)
            gather_ref[:, k * LANES : (k + 1) * LANES] = hit.astype(f32).astype(bf16)
            index = lax.broadcasted_iota(jnp.int32, (block, spread), 0)
            hit = where_of(index, k) == lax.broadcasted_iota(jnp.int32, (block, spread), 1)
            scatter_ref[k] = hit.astype(f32).astype(bf16)

    tile = 2 * LANES

    def above(size):
        return (
            lax.broadcasted_iota(jnp.int32, (size, size), 0)
            > lax.broadcasted_iota(jnp.int32, (size, size), 1)
        ).astype(bf16)

    lane = lax.broadcasted_iota(jnp.int32, (rows, LANES), 1)
    offsets = (0, heads_a)
    fill = jnp.zeros((LANES - stops_own.shape[0], stops_own.shape[1]), f32)

    def weigh(mine, keys, stop, scale, upper, valid, carry):
        score = lax.dot_general(mine, keys, (((1,), (1,)), ((), ())), preferred_element_type=f32)
        score = score * scale + stop
        fail = jnp.log2(1.0 + jnp.exp2(jnp.minimum(score, 100.0)))
        fail = jnp.maximum(fail, score)
        hit = score - fail
        if valid is not None:
            fail = jnp.where(valid, fail, 0.0)
        after = dot(fail.astype(bf16), upper)
        weight = jnp.exp2(hit - after if carry is None else hit - after - carry)
        if valid is not None:
            weight = jnp.where(valid, weight, 0.0)
        spent = after[:, :1] + fail[:, :1]
        return weight.astype(bf16), spent if carry is None else carry + spent

    def merge(parts, size):
        merged = parts[0]
        for h in range(1, len(parts)):
            merged = jnp.where(lane // size >= h, parts[h], merged)
        return merged

    def at_home(g):
        size = groups[g][1]
        heads = LANES // size
        scale = LOG2E * size ** (-0.5)
        upper = above(2 * rows)
        valid = lax.broadcasted_iota(jnp.int32, (rows, 2 * rows), 1) < (
            lax.broadcasted_iota(jnp.int32, (rows, 2 * rows), 0) + c * rows
        )
        stop_all = jnp.concatenate([stops_own[...], fill], axis=0).T[:rows]
        for t in (3 * g + 1, 3 * g + 2):
            landed(near[t].at[pl.ds(pl.multiple_of((1 - c) * rows, rows), rows), :], nrecv.at[t])
        for u in range(groups[g][0]):
            lanes = slice(u * LANES, (u + 1) * LANES)
            query = near[3 * g][:, lanes]
            keys, values = near[3 * g + 1][:, lanes], near[3 * g + 2][:, lanes]
            parts, factors = [], []
            for h in range(heads):
                head = offsets[g] + u * heads + h
                stop = stop_all[:, head : head + 1] * LOG2E
                mine = query * ((lane // size) == h).astype(bf16) if heads > 1 else query
                weight, spent = weigh(mine, keys, stop, scale, upper, valid, None)
                parts.append(dot(weight, values))
                factors.append(jnp.exp2(-spent))
            home[2 * g][:, lanes] = merge(parts, size)
            home[2 * g + 1][:, lanes] = merge(
                [jnp.broadcast_to(f, (rows, LANES)) for f in factors], size
            )

    tables()
    at_home(0)
    push(1)
    at_home(1)
    for chip in range(ends):
        relay(0, chip)
    upper = above(tile)
    backs = []
    steps = [(g, m) for g in range(2) for m in range(1, nz)]
    for g, m in steps:
        relayed(g, m - 1)
        size = groups[g][1]
        heads = LANES // size
        q_ref, k_ref, v_ref = full[3 * g : 3 * g + 3]
        scale = LOG2E * size ** (-0.5)
        block_q = 2 * m + c
        for t in names[g][0]:
            landed(spot(t, block_q), frecv.at[m, t])
        query = q_ref[pl.ds(pl.multiple_of(block_q * rows, rows), rows), :]
        lines = stops_own.shape[0]
        stop_t = full[6][pl.ds(pl.multiple_of(block_q * lines, lines), lines), :]
        stop_all = jnp.concatenate([stop_t, fill], axis=0).T[:rows]
        reach = 2 * m * rows
        count = -(-reach // tile)
        parts = []
        for h in range(heads):
            head = offsets[g] + z * heads + h
            stop = jnp.sum(jnp.where(lane == head, stop_all, 0.0), axis=1, keepdims=True) * LOG2E
            mine = query * ((lane // size) == h).astype(bf16) if heads > 1 else query
            carry = jnp.zeros((rows, 1), f32)
            total = jnp.zeros((rows, LANES), f32)
            for i in range(count):
                if (g, m, h, i) == (0, ends, heads - 1, count // 2):
                    for chip in range(ends):
                        relay(1, chip)
                stop_at = reach - tile * i
                start = max(stop_at - tile, 0)
                wide = stop_at - start
                weight, carry = weigh(
                    mine, k_ref[start:stop_at], stop, scale, upper[:wide, :wide], None, carry
                )
                total = total + dot(weight, v_ref[start:stop_at])
            parts.append(total)
        made[g][m] = merge(parts, size).astype(bf16)
        place = attended[g].at[:, pl.ds(pl.multiple_of(z * LANES, LANES), LANES)]
        backs.append((g, m))

        @pl.when(m != z)
        def _(g=g, m=m, place=place, block_q=block_q):
            pltpu.make_async_remote_copy(
                src_ref=made[g].at[m],
                dst_ref=place,
                send_sem=osend.at[g, m],
                recv_sem=orecv.at[g, z],
                device_id={"sp": block_q},
                device_id_type=MESH,
            ).start()

        @pl.when(m == z)
        def _(g=g, m=m, place=place):
            pltpu.make_async_copy(made[g].at[m], place, orecv.at[g, z]).start()

    loads[0].wait()
    loads[1].wait()
    loads[2].wait()

    def columns(which, wide):
        return pl.ds(pl.multiple_of(which * wide, wide), wide)

    peers = [lax.rem(col + d, n_tp) for d in range(1, n_tp)] + [col]
    for g, weights in enumerate((w_out_a, w_out_b)):
        @pl.when(z == 0)
        def _(g=g):
            left_refs[g][...] = home[2 * g][...].astype(bf16)

        @pl.when(z > 0)
        def _(g=g):
            for u in range(groups[g][0]):
                lanes = slice(u * LANES, (u + 1) * LANES)
                landed(attended[g].at[:, lanes], orecv.at[g, u])
                far = home[2 * g + 1][:, lanes] * attended[g][:, lanes].astype(f32)
                left_refs[g][:, lanes] = (home[2 * g][:, lanes] + far).astype(bf16)

        left = left_refs[g][...]
        for i, peer in enumerate(peers):
            term = dot(left, weights[:, columns(peer, width)])
            if g == 0:
                partial[i] = term
                continue
            part_out[i] = (partial[i] + term).astype(bf16)
            if i < n_tp - 1:
                remote(part_out.at[i], part_in.at[i], xsend.at[i], xrecv.at[i], {"tp": peer})
    resid = resid_ref[...].astype(f32)
    mixed = part_out[n_tp - 1].astype(f32)
    for i in range(n_tp - 1):
        landed(part_in.at[i], xrecv.at[i])
        mixed = mixed + part_in[i].astype(f32)

    shaped = mixed * mix_gain[...]
    sums = jnp.zeros((rows, LANES), f32)
    for i, term in enumerate((mixed * mixed, resid * resid, resid * shaped, shaped * shaped)):
        sums = jnp.where(lane == i, jnp.sum(term, axis=1, keepdims=True), sums)
    if tall_rows > rows:
        sums = jnp.concatenate([sums, jnp.zeros((tall_rows - rows, LANES), f32)], axis=0)
    stats_out[...] = sums.T[:8]
    for d in range(1, n_tp):
        remote(
            stats_out, stats_in.at[d - 1], tsend.at[d - 1], trecv.at[d - 1], {"tp": peers[d - 1]}
        )
    sums = stats_out[...]
    for d in range(1, n_tp):
        landed(stats_in.at[d - 1], trecv.at[d - 1])
        sums = sums + stats_in[d - 1]
    sums = jnp.concatenate([sums, jnp.zeros((LANES - 8, tall_rows), f32)], axis=0).T[:rows]
    model = width * n_tp
    scale = lax.rsqrt(sums[:, 0:1] / model + epsilon)
    stream = (resid + shaped * scale).astype(bf16)
    square = sums[:, 1:2] + scale * (2.0 * sums[:, 2:3] + scale * sums[:, 3:4])
    square = jnp.maximum(square, 0.0)
    stream = stream.astype(f32)
    result_ref[...] = stream
    normed = stream * lax.rsqrt(square / model + epsilon) * ffn_gain[...]
    normed_ref[...] = normed.astype(bf16)

    chips = [flip(z, o) for o in order]
    shared = len(chips)
    seat = lax.broadcasted_iota(jnp.int32, (block, rows), 0)
    for i, o in enumerate(order):
        for k in range(2):
            peer = chips[i] * 2 + lax.rem(c + k, 2)
            seats = (seat + peer * block).astype(f32)
            chosen = seats == slot_rows[0]
            for slot in slot_rows[1:]:
                chosen = jnp.logical_or(chosen, seats == slot)
            picked = dot(chosen.astype(f32).astype(bf16), normed_ref[...])
            out_ref[2 * i + k] = picked.astype(bf16)
            if o == 0 and k == 0:
                pltpu.make_async_copy(out_ref.at[2 * i + k], arrived.at[me], drecv.at[me]).start()
            else:
                remote(
                    out_ref.at[2 * i + k],
                    arrived.at[me],
                    dsend.at[2 * i + k],
                    drecv.at[me],
                    {"sp": peer},
                )

    def buffers(i):
        if i == shared:
            return s_pre, s_pre_in, s_hid
        return pre.at[i], pre_in.at[i], hid.at[i]

    def first(i):
        here, there, _ = buffers(i)
        if i == shared:
            loads[6].wait()
            loads[7].wait()
            for k, weight in enumerate((sg_ref, su_ref)):
                here[k] = dot(normed_ref[...], weight[...]).astype(bf16)
        else:
            grouped = None
            for k in range(2):
                source = chips[i] * 2 + k
                landed(arrived.at[source], drecv.at[source])
                term = dot(gather_ref[:, k * LANES : k * LANES + block], arrived[source])
                grouped = term if grouped is None else grouped + term
            grouped = grouped.astype(bf16)
            tall = grouped.shape[0] // experts
            if i == 0:
                loads[3].wait()
                loads[4].wait()
            for k, weight in enumerate((w_gate, w_up)):
                terms = [
                    dot(grouped[e * tall : (e + 1) * tall], weight[e]).astype(bf16)
                    for e in range(experts)
                ]
                spread_rows = jnp.concatenate(terms, axis=0)
                here[k] = jnp.concatenate(
                    [dot(scatter_ref[j], spread_rows) for j in range(2)], axis=0
                ).astype(bf16)
        for d in range(1, n_tp):
            for k in range(2):
                remote(
                    here.at[k, :, columns(peers[d - 1], part)],
                    there.at[d - 1, k],
                    psend.at[i, d - 1, k],
                    precv.at[i, d - 1, k],
                    {"tp": peers[d - 1]},
                )

    def second(i):
        here, there, whole = buffers(i)
        sums = []
        for k in range(2):
            total = here[k, :, columns(col, part)].astype(f32)
            for d in range(1, n_tp):
                landed(there.at[d - 1, k], precv.at[i, d - 1, k])
                total = total + there[d - 1, k].astype(f32)
            sums.append(total)
        whole[:, columns(col, part)] = (sums[0] / (1.0 + jnp.exp(-sums[0])) * sums[1]).astype(bf16)
        for d in range(1, n_tp):
            mine = whole.at[:, columns(col, part)]
            remote(mine, mine, hsend.at[i, d - 1], hrecv.at[i, d - 1], {"tp": peers[d - 1]})

    kept = []

    def third(i):
        _, _, whole = buffers(i)
        for d in range(1, n_tp):
            source = lax.rem(col + n_tp - d, n_tp)
            landed(whole.at[:, columns(source, part)], hrecv.at[i, d - 1])
        if i == shared:
            loads[8].wait()
            result_ref[...] = result_ref[...] + dot(whole[...], sd_ref[...])
            return
        hidden = whole[...]
        grouped = dot(gather_ref[:, :block], hidden[:block]) + dot(
            gather_ref[:, LANES : LANES + block], hidden[block:]
        )
        grouped = grouped.astype(bf16)
        tall = grouped.shape[0] // experts
        if i == 0:
            loads[5].wait()
        terms = [
            dot(grouped[e * tall : (e + 1) * tall], w_down[e]).astype(bf16) for e in range(experts)
        ]
        terms = jnp.concatenate(terms, axis=0)
        for k in range(2):
            source = chips[i] * 2 + k
            made_back[i, k] = dot(scatter_ref[k], terms).astype(bf16)
            if order[i] == 0:

                @pl.when(source != me)
                def _():
                    pltpu.make_async_remote_copy(
                        src_ref=made_back.at[i, k],
                        dst_ref=returned.at[me],
                        send_sem=bsend.at[i, k],
                        recv_sem=brecv.at[me],
                        device_id={"sp": source},
                        device_id_type=MESH,
                    ).start()

                @pl.when(source == me)
                def _():
                    pltpu.make_async_copy(made_back.at[i, k], returned.at[me], brecv.at[me]).start()

                kept.append((i, k, source))
            else:
                remote(
                    made_back.at[i, k],
                    returned.at[me],
                    bsend.at[i, k],
                    brecv.at[me],
                    {"sp": source},
                )

    top_count = routes_ref.shape[0]
    turned = aux[...].T[:rows]
    taken = lax.broadcasted_iota(jnp.int32, (rows, block), 1)

    def combine(i):
        total = result_ref[...]
        for k in range(2):
            source = chips[i] * 2 + k
            landed(returned.at[source], brecv.at[source])
            seats = (taken + source * block).astype(f32)
            gated = jnp.zeros(seats.shape, f32)
            for t in range(top_count):
                gate = turned[:, top_count + t : top_count + t + 1]
                gated = gated + jnp.where(seats == turned[:, t : t + 1], gate, 0.0)
            high = gated.astype(bf16)
            low = (gated - high.astype(f32)).astype(bf16)
            total = total + dot(high, returned[source]) + dot(low, returned[source])
        result_ref[...] = total

    first(shared)
    first(0)
    second(shared)
    for i in range(1, shared + 2):
        if i < shared:
            first(i)
        if i <= shared:
            second(i - 1)
        if i == 1:
            third(shared)
        else:
            third(i - 2)
        if i >= 4:
            combine(i - 4)
    for i in range(max(shared - 2, 0), shared):
        combine(i)
    for copy in sends:
        copy.wait_send()
    pushed(0)
    pushed(1)
    for g, m in backs:

        @pl.when(m != z)
        def _(g=g, m=m):
            landed(made[g].at[m], osend.at[g, m])

    for i, k, source in kept:

        @pl.when(source != me)
        def _(i=i, k=k):
            landed(made_back.at[i, k], bsend.at[i, k])


def layer(n_sp, n_tp, groups, capacity, arrays, small, large):
    f32, bf16 = jnp.float32, jnp.bfloat16
    rows = arrays[0].shape[0]
    resid, w_gate = large[2], large[3]
    width = resid.shape[1]
    experts, hidden_width = w_gate.shape[0], w_gate.shape[2]
    block = experts * capacity
    nz = n_sp // 2
    order = tuple(range(nz // 2, nz)) + tuple(range(nz // 2 - 1, -1, -1))
    wide = -(-rows // LANES) * LANES
    lines = -(-(small[0].shape[0] + small[1].shape[0]) // 8) * 8
    tall = -(-2 * capacity // 16) * 16
    part = hidden_width // n_tp
    dma = pltpu.SemaphoreType.DMA
    vmem = pltpu.VMEM
    anywhere = pl.BlockSpec(memory_space=pl.ANY)
    scratch = (
        [vmem((n_sp * rows, LANES), bf16)] * 6
        + [vmem((n_sp * lines, wide), f32)]
        + [vmem(((1 if t % 3 == 0 else 2) * rows, a.shape[1]), bf16) for t, a in enumerate(arrays)]
        + [vmem((rows, units * LANES), f32) for units, _ in groups for _ in range(2)]
        + [vmem((rows, units * LANES), bf16) for units, _ in groups]
        + [vmem((nz, rows, LANES), bf16)] * 2
        + [vmem((rows, units * LANES), bf16) for units, _ in groups]
        + [vmem(a.shape, a.dtype) for a in large]
        + [
            vmem((lines, wide), f32),
            vmem((n_tp, rows, width), f32),
            vmem((n_tp, rows, width), bf16),
            vmem((n_tp - 1, rows, width), bf16),
            vmem((LANES, wide), f32),
            vmem((8, wide), f32),
            vmem((n_tp - 1, 8, wide), f32),
            vmem((rows, width), bf16),
        ]
        + [
            vmem((n_sp, block, width), bf16),
            vmem((n_sp, block, width), bf16),
            vmem((n_sp, block, width), bf16),
            vmem((nz, 2, block, width), bf16),
            vmem((nz, 2, 2 * block, hidden_width), bf16),
            vmem((nz, n_tp - 1, 2, 2 * block, part), bf16),
            vmem((nz, 2 * block, hidden_width), bf16),
            vmem((2, rows, hidden_width), bf16),
            vmem((n_tp - 1, 2, rows, part), bf16),
            vmem((rows, hidden_width), bf16),
        ]
        + [vmem((experts * tall, 2 * LANES), bf16), vmem((2, block, experts * tall), bf16)]
        + [dma((len(large) + len(arrays),))]
        + [dma((nz, 7))] * 4
        + [dma((2, nz))] * 2
        + [dma((n_tp - 1,))] * 4
        + [dma((n_sp,)), dma((n_sp,)), dma((nz, 2)), dma((n_sp,))]
        + [dma((nz + 1, n_tp - 1, 2))] * 2
        + [dma((nz + 1, n_tp - 1))] * 2
        + [dma((6,))] * 2
    )
    return pl.pallas_call(
        functools.partial(layer_kernel, n_sp, n_tp, groups, capacity, order),
        out_shape=pltpu.VMEM((rows, width), f32),
        in_specs=[anywhere] * 6 + [VM] * 6 + [anywhere] * 9,
        out_specs=VM,
        scratch_shapes=scratch,
        compiler_params=params(9),
        name="layer",
    )(*arrays, *small, *large)


def shards(
    n_sp,
    n_tp,
    query_a,
    key_a,
    value_a,
    query_b,
    key_b,
    value_b,
    stop_a,
    stop_b,
    out_a,
    out_b,
    resid,
    mix_gain,
    ffn_gain,
    routes,
    gates,
    exp_gate,
    exp_up,
    exp_down,
    sh_gate,
    sh_up,
    sh_down,
):
    f32, bf16 = jnp.float32, jnp.bfloat16
    rows = query_a.shape[0]
    heads_a, heads_b = stop_a.shape[1], stop_b.shape[1]
    units_a, units_b = query_a.shape[1] // LANES, query_b.shape[1] // LANES
    width = resid.shape[1]
    model = width * n_tp

    local_experts = exp_gate.shape[0]
    experts = local_experts * n_sp
    top_count = routes.shape[1]
    capacity = max(1, (3 * rows * top_count + 2 * experts - 1) // (2 * experts))
    block = local_experts * capacity
    hidden_width = exp_gate.shape[2]
    groups = ((units_a, query_a.shape[1] // heads_a), (units_b, query_b.shape[1] // heads_b))
    fused = (
        (hidden_width // n_tp) % LANES == 0
        and width % LANES == 0
        and block % 8 == 0
        and block <= LANES
        and exp_gate.shape == exp_down.shape
        and all(2 * units == n_sp for units, _ in groups)
        and (n_sp // 2) & (n_sp // 2 - 1) == 0
        and 2 * rows <= 4 * LANES
        and 2 * rows % LANES == 0
        and rows % 16 == 0
    )
    if fused:
        arrays = (query_a, key_a, value_a, query_b, key_b, value_b)
        small = (stop_a.T, stop_b.T, routes.T, gates.T, mix_gain[None, :], ffn_gain[None, :])
        large = (out_a, out_b, resid, exp_gate, exp_up, exp_down, sh_gate, sh_up, sh_down)
        return layer(n_sp, n_tp, groups, capacity, arrays, small, large).astype(bf16)

    flat_routes = routes.reshape(-1)
    onehot = (flat_routes[:, None] == jnp.arange(experts, dtype=jnp.int32)[None, :]).astype(f32)
    pairs = rows * top_count
    before = (jnp.arange(pairs)[:, None] > jnp.arange(pairs)[None, :]).astype(bf16)
    earlier = jnp.dot(before, onehot.astype(bf16), preferred_element_type=f32)
    slot = flat_routes * capacity + jnp.sum(earlier * onehot, axis=1).astype(jnp.int32)
    slot = slot.reshape(rows, top_count)
    slots = jnp.arange(experts * capacity, dtype=jnp.int32)
    chosen = slot[:, :, None] == slots[None, None, :]
    chooser = jnp.sum(chosen.astype(f32), axis=1).astype(bf16)
    gated = jnp.sum(jnp.where(chosen, gates[:, :, None], 0.0), axis=1)
    gated_high = gated.astype(bf16)
    gated_low = (gated - gated_high.astype(f32)).astype(bf16)

    stops = jnp.concatenate([stop_a, stop_b], axis=1)
    lines = -(-stops.shape[1] // 8) * 8
    wide = -(-rows // LANES) * LANES
    stops = jnp.pad(stops.T, ((0, lines - stops.shape[1]), (0, wide - rows)))
    arrays = (query_a, key_a, value_a, query_b, key_b, value_b, stops)
    attended_a, attended_b = stick(n_sp, rows, arrays, groups, (0, heads_a), 0)

    partial_value = jnp.dot(attended_a, out_a, preferred_element_type=f32)
    partial_value = partial_value + jnp.dot(attended_b, out_b, preferred_element_type=f32)
    (pieces,) = exchange("tp", n_tp, (partial_value.astype(bf16),), ("cols",), 2)
    mixed = jnp.sum(pieces.astype(f32), axis=0)
    resid_f = resid.astype(f32)
    shaped = mixed * mix_gain[None, :]
    sums = jnp.stack(
        [
            jnp.sum(mixed * mixed, axis=1),
            jnp.sum(resid_f * resid_f, axis=1),
            jnp.sum(resid_f * shaped, axis=1),
            jnp.sum(shaped * shaped, axis=1),
        ]
    )
    sums = jnp.pad(sums, ((0, 4), (0, wide - rows)))
    (sums,) = exchange("tp", n_tp, (sums,), ("all",), 3)
    sums = jnp.sum(sums, axis=0)[:4, :rows]
    scale = lax.rsqrt(sums[0] / model + epsilon)
    stream = (resid_f + shaped * scale[:, None]).astype(bf16)
    square = jnp.maximum(sums[1] + scale * (2.0 * sums[2] + scale * sums[3]), 0.0)
    stream_f = stream.astype(f32)
    normed = (stream_f * lax.rsqrt(square / model + epsilon)[:, None] * ffn_gain[None, :]).astype(bf16)

    outgoing = lax.dot_general(chooser, normed, (((0,), (0,)), ((), ())), preferred_element_type=f32)
    outgoing = outgoing.astype(bf16).reshape(n_sp, local_experts * capacity, width)
    (arrived,) = exchange("sp", n_sp, (outgoing,), ("lead",), 4)
    arrived = arrived.reshape(n_sp, local_experts, capacity, width)
    arrived = jnp.transpose(arrived, (1, 0, 2, 3)).reshape(local_experts, n_sp * capacity, width)

    shared_parts = [
        jnp.dot(normed, w, preferred_element_type=f32).astype(bf16) for w in (sh_gate, sh_up)
    ]
    expert_parts = [
        jnp.einsum("erd,edf->erf", arrived, w, preferred_element_type=f32)
        .astype(bf16)
        .reshape(local_experts * n_sp * capacity, -1)
        for w in (exp_gate, exp_up)
    ]
    parts = exchange("tp", n_tp, (*expert_parts, *shared_parts), ("cols",) * 4, 5)
    gate_pre, up_pre, shared_gate, shared_up = [jnp.sum(p.astype(f32), axis=0) for p in parts]
    hidden = (jax.nn.silu(gate_pre) * up_pre).astype(bf16)
    shared_hidden = (jax.nn.silu(shared_gate) * shared_up).astype(bf16)
    hidden, shared_hidden = exchange("tp", n_tp, (hidden, shared_hidden), ("side",) * 2, 6)

    shared_out = jnp.dot(shared_hidden, sh_down, preferred_element_type=f32)
    hidden = hidden.reshape(local_experts, n_sp * capacity, -1)
    produced = jnp.einsum("erf,efd->erd", hidden, exp_down, preferred_element_type=f32).astype(bf16)
    produced = produced.reshape(local_experts, n_sp, capacity, width)
    produced = jnp.transpose(produced, (1, 0, 2, 3)).reshape(n_sp, local_experts * capacity, width)
    (returned,) = exchange("sp", n_sp, (produced,), ("lead",), 7)
    flat_back = returned.reshape(experts * capacity, width)
    routed = jnp.dot(gated_high, flat_back, preferred_element_type=f32)
    routed = routed + jnp.dot(gated_low, flat_back, preferred_element_type=f32)
    moe = routed + shared_out
    return (stream_f + moe).astype(bf16)


def solution(mesh):
    return jax.shard_map(
        functools.partial(shards, mesh.shape["sp"], mesh.shape["tp"]),
        mesh=mesh,
        in_specs=(
            P("sp", "tp"),
            P("sp", "tp"),
            P("sp", "tp"),
            P("sp", "tp"),
            P("sp", "tp"),
            P("sp", "tp"),
            P("sp", "tp"),
            P("sp", "tp"),
            P("tp", None),
            P("tp", None),
            P("sp", "tp"),
            P("tp"),
            P("tp"),
            P("sp", None),
            P("sp", None),
            P("sp", "tp", None),
            P("sp", "tp", None),
            P("sp", None, "tp"),
            P("tp", None),
            P("tp", None),
            P(None, "tp"),
        ),
        out_specs=P("sp", "tp"),
        check_vma=False,
    )
```

```python
import functools
import math

import jax
import jax.numpy as jnp
import numpy as np
from jax import lax
from jax.experimental import pallas as pl
from jax.experimental.pallas import tpu as pltpu
from jax.sharding import PartitionSpec as P

MESH = pl.DeviceIdType.MESH
LANES = 128
LOG2E = 1.4426950408889634
epsilon = 1e-06
VM = pl.BlockSpec(memory_space=pltpu.VMEM)


def greet(axis, peers):
    barrier = pltpu.get_barrier_semaphore()
    for peer in peers:
        pl.semaphore_signal(barrier, inc=1, device_id={axis: peer}, device_id_type=MESH)
    pl.semaphore_wait(barrier, len(peers))


def params(cid):
    return pltpu.CompilerParams(
        collective_id=cid, has_side_effects=True, vmem_limit_bytes=56 * 1024 * 1024
    )


def snake(r, j, m):
    return m * r + (j if m % 2 == 0 else r - 1 - j)


def stick_kernel(n, rows, groups, offsets, *refs):
    g_count = len(groups)
    count = 3 * g_count + 1
    ins, outs = refs[:count], refs[count : count + g_count]
    full = refs[count + g_count : 2 * count + g_count]
    made = refs[2 * count + g_count : 2 * count + 2 * g_count]
    send, recv, rsend, rrecv, own, bsend, brecv = refs[2 * count + 2 * g_count :]
    me = lax.axis_index("sp")
    nz = n // 2
    z, c = me // 2, lax.rem(me, 2)
    partner = z * 2 + 1 - c
    places = [lax.rem(z + d, nz) for d in range(nz)]
    greet("sp", [lax.rem(me + d, n) for d in range(1, n)])
    order = [count - 1] + list(range(count - 1))

    def piece(t, place):
        if t == count - 1:
            return ins[t]
        unit = (2 * place) // (n // groups[t // 3][0])
        return ins[t].at[:, pl.ds(pl.multiple_of(unit * LANES, LANES), LANES)]

    def spot(t, source):
        tall = ins[t].shape[0]
        return full[t].at[pl.ds(pl.multiple_of(source * tall, tall), tall), :]

    def remote(source, target, send_sem, recv_sem, device):
        copy = pltpu.make_async_remote_copy(
            src_ref=source,
            dst_ref=target,
            send_sem=send_sem,
            recv_sem=recv_sem,
            device_id={"sp": device},
            device_id_type=MESH,
        )
        copy.start()
        return copy

    first, relays, local = {}, {}, {}
    for t in order:
        for d in range(1, nz):
            first[d, t] = remote(
                piece(t, places[d]), spot(t, me), send.at[d, t], recv.at[d, t], places[d] * 2 + c
            )
        relays[0, t] = remote(piece(t, z), spot(t, me), rsend.at[0, t], rrecv.at[0, t], partner)
        local[t] = pltpu.make_async_copy(piece(t, z), spot(t, me), own.at[t])
        local[t].start()

    def relay(d, t):
        source = lax.rem(z + nz - d, nz) * 2 + c
        first[d, t].wait_recv()
        relays[d, t] = remote(
            spot(t, source), spot(t, source), rsend.at[d, t], rrecv.at[d, t], partner
        )

    def arrive(t):
        local[t].wait()
        for d in range(nz):
            relays[d, t].wait_recv()

    group_arrays = lambda g: ([count - 1] if g == 0 else []) + [3 * g, 3 * g + 1, 3 * g + 2]
    for d in range(1, nz):
        for t in group_arrays(0):
            relay(d, t)

    tile = 2 * LANES
    upper = (
        lax.broadcasted_iota(jnp.int32, (tile, tile), 0)
        > lax.broadcasted_iota(jnp.int32, (tile, tile), 1)
    ).astype(jnp.bfloat16)
    lane = lax.broadcasted_iota(jnp.int32, (rows, LANES), 1)
    column = lax.broadcasted_iota(jnp.int32, (rows, tile), 1)
    line = lax.broadcasted_iota(jnp.int32, (rows, tile), 0)
    backs = []
    for g in range(g_count):
        units, size = groups[g]
        q_ref, k_ref, v_ref = full[3 * g : 3 * g + 3]
        r = n // units
        unit, j = me // r, lax.rem(me, r)
        heads = LANES // size
        scale = LOG2E * size ** (-0.5)
        for t in group_arrays(g):
            arrive(t)
        pending = []
        if g + 1 < g_count:
            pending = [(d, t) for d in range(1, nz) for t in group_arrays(g + 1)]
        for m in range(n // r):
            block = snake(r, j, m)
            last = lambda b: ((b + 1) * rows - 1) // tile
            counts = [last(snake(r, jj, m)) + 1 for jj in range(r)]
            query = q_ref[pl.ds(pl.multiple_of(block * rows, rows), rows), :]
            lines = ins[count - 1].shape[0]
            stop_t = full[count - 1][pl.ds(pl.multiple_of(block * lines, lines), lines), :]
            fill = jnp.zeros((LANES - lines, stop_t.shape[1]), jnp.float32)
            stop_all = jnp.concatenate([stop_t, fill], axis=0).T[:rows]
            parts = []
            for h in range(heads):
                head = offsets[g] + unit * heads + h
                stop = jnp.sum(jnp.where(lane == head, stop_all, 0.0), axis=1, keepdims=True) * LOG2E
                if heads > 1:
                    mine = query * ((lane // size) == h).astype(jnp.bfloat16)
                else:
                    mine = query
                carry = jnp.zeros((rows, 1), jnp.float32)
                total = jnp.zeros((rows, LANES), jnp.float32)
                for i in range(max(counts)):
                    where_tile = (block * rows + rows - 1) // tile - i
                    masked = i < 2 or i >= min(counts)
                    start = pl.multiple_of(jnp.maximum(where_tile, 0) * tile, tile)
                    keys = k_ref[pl.ds(start, tile), :]
                    values = v_ref[pl.ds(start, tile), :]
                    score = lax.dot_general(
                        mine, keys, (((1,), (1,)), ((), ())), preferred_element_type=jnp.float32
                    )
                    score = score * scale + stop
                    small = jnp.log2(1.0 + jnp.exp2(-jnp.abs(score)))
                    fail = jnp.maximum(score, 0.0) + small
                    hit = score - fail
                    if masked:
                        valid = column + where_tile * tile < line + block * rows
                        if i >= min(counts):
                            valid = jnp.logical_and(valid, where_tile >= 0)
                        fail = jnp.where(valid, fail, 0.0)
                    high = fail.astype(jnp.bfloat16)
                    low = (fail - high.astype(jnp.float32)).astype(jnp.bfloat16)
                    after = jnp.dot(high, upper, preferred_element_type=jnp.float32) + jnp.dot(
                        low, upper, preferred_element_type=jnp.float32
                    )
                    weight = jnp.exp2(hit - after - carry)
                    if masked:
                        weight = jnp.where(valid, weight, 0.0)
                    carry = carry + after[:, :1] + fail[:, :1]
                    total = total + jnp.dot(
                        weight.astype(jnp.bfloat16), values, preferred_element_type=jnp.float32
                    )
                parts.append(total)
            merged = parts[0]
            for h in range(1, heads):
                merged = jnp.where(lane // size >= h, parts[h], merged)
            made[g][m] = merged.astype(jnp.bfloat16)
            place = outs[g].at[:, pl.ds(pl.multiple_of(unit * LANES, LANES), LANES)]

            @pl.when(block != me)
            def _():
                pltpu.make_async_remote_copy(
                    src_ref=made[g].at[m],
                    dst_ref=place,
                    send_sem=bsend.at[g, m],
                    recv_sem=brecv.at[g, unit],
                    device_id={"sp": block},
                    device_id_type=MESH,
                ).start()

            @pl.when(block == me)
            def _():
                pltpu.make_async_copy(made[g].at[m], place, bsend.at[g, m]).start()

            share = -(-len(pending) // (n // r - m))
            for d, t in pending[:share]:
                relay(d, t)
            pending = pending[share:]

    for g in range(g_count):
        r = n // groups[g][0]
        turn, rest = me // r, lax.rem(me, r)
        owner = jnp.where(lax.rem(turn, 2) == 0, rest, r - 1 - rest)
        for u in range(groups[g][0]):

            @pl.when(u * r + owner != me)
            def _(g=g, u=u):
                place = outs[g].at[:, pl.ds(u * LANES, LANES)]
                pltpu.make_async_copy(place, place, brecv.at[g, u]).wait()

        unit = me // r
        place = outs[g].at[:, pl.ds(pl.multiple_of(unit * LANES, LANES), LANES)]
        for m in range(groups[g][0]):
            pltpu.make_async_copy(made[g].at[m], place, bsend.at[g, m]).wait()
    for copy in first.values():
        copy.wait_send()
    for copy in relays.values():
        copy.wait_send()


def stick(n, rows, arrays, groups, offsets, cid):
    k, g_count = len(arrays), len(groups)
    nz, top = n // 2, max(units for units, _ in groups)
    dma = pltpu.SemaphoreType.DMA
    return pl.pallas_call(
        functools.partial(stick_kernel, n, rows, groups, offsets),
        out_shape=tuple(
            jax.ShapeDtypeStruct((rows, units * LANES), jnp.bfloat16) for units, _ in groups
        ),
        in_specs=[VM] * k,
        out_specs=[VM] * g_count,
        scratch_shapes=[
            pltpu.VMEM((n * a.shape[0], LANES if i < k - 1 else a.shape[1]), a.dtype)
            for i, a in enumerate(arrays)
        ]
        + [pltpu.VMEM((units, rows, LANES), jnp.bfloat16) for units, _ in groups]
        + [dma((nz, k))] * 4
        + [dma((k,)), dma((g_count, top)), dma((g_count, top))],
        compiler_params=params(cid),
        name="stick",
    )(*arrays)


def exchange_kernel(axis, n, modes, *refs):
    count = len(modes)
    ins, outs = refs[:count], refs[count : 2 * count]
    send, recv = refs[2 * count :]
    me = lax.axis_index(axis)
    greet(axis, [lax.rem(me + d, n) for d in range(1, n)])

    def ends(t, peer):
        if modes[t] == "lead":
            return ins[t].at[peer], outs[t].at[me]
        if modes[t] == "cols":
            width = ins[t].shape[1] // n
            return ins[t].at[:, pl.ds(pl.multiple_of(peer * width, width), width)], outs[t].at[me]
        if modes[t] == "all":
            return ins[t], outs[t].at[me]
        width = ins[t].shape[1]
        return ins[t], outs[t].at[:, pl.ds(pl.multiple_of(me * width, width), width)]

    copies = []
    for d in range(1, n):
        peer = lax.rem(me + d, n)
        for t in range(count):
            source, target = ends(t, peer)
            copies.append(
                pltpu.make_async_remote_copy(
                    src_ref=source,
                    dst_ref=target,
                    send_sem=send.at[d, t],
                    recv_sem=recv.at[d, t],
                    device_id={axis: peer},
                    device_id_type=MESH,
                )
            )
            copies[-1].start()
    for t in range(count):
        source, target = ends(t, me)
        copies.append(pltpu.make_async_copy(source, target, send.at[0, t]))
        copies[-1].start()
    for copy in copies:
        copy.wait()


def exchange(axis, n, arrays, modes, cid):
    def shape(a, mode):
        if mode == "lead":
            return a.shape
        if mode == "cols":
            return (n, a.shape[0], a.shape[1] // n)
        if mode == "all":
            return (n,) + a.shape
        return (a.shape[0], a.shape[1] * n)

    if modes[0] == "cols" and any((a.shape[1] // n) % LANES for a in arrays):
        cut = [jnp.transpose(a.reshape(a.shape[0], n, -1), (1, 0, 2)) for a in arrays]
        return exchange(axis, n, cut, ("lead",) * len(cut), cid)
    if modes[0] == "side" and any(a.shape[1] % LANES for a in arrays):
        stacked = exchange(axis, n, arrays, ("all",) * len(arrays), cid)
        return [jnp.transpose(a, (1, 0, 2)).reshape(a.shape[1], -1) for a in stacked]
    k = len(arrays)
    return pl.pallas_call(
        functools.partial(exchange_kernel, axis, n, modes),
        out_shape=tuple(jax.ShapeDtypeStruct(shape(a, m), a.dtype) for a, m in zip(arrays, modes)),
        in_specs=[VM] * k,
        out_specs=[VM] * k,
        scratch_shapes=[pltpu.SemaphoreType.DMA((n, k))] * 2,
        compiler_params=params(cid),
        name="exchange",
    )(*arrays)


def flip(z, offset):
    other, bit = z, 1
    while bit <= offset:
        if offset & bit:
            other = other + bit - 2 * bit * lax.rem(z // bit, 2)
        bit *= 2
    return other


def layer_kernel(n_sp, n_tp, groups, capacity, order, *refs):
    f32, bf16 = jnp.float32, jnp.bfloat16
    pieces, refs = refs[:6], refs[6:]
    (stop_a, stop_b, routes_ref, gates_ref, mix_gain, ffn_gain), refs = refs[:6], refs[6:]
    large, refs = refs[:9], refs[9:]
    result_ref, refs = refs[0], refs[1:]
    full, refs = refs[:7], refs[7:]
    near, refs = refs[:6], refs[6:]
    home, refs = refs[:4], refs[4:]
    left_refs, refs = refs[:2], refs[2:]
    made, refs = refs[:2], refs[2:]
    attended, refs = refs[:2], refs[2:]
    held, refs = refs[:9], refs[9:]
    (stops_own, partial, part_out, part_in, aux, stats_out, stats_in, normed_ref), refs = (
        refs[:8],
        refs[8:],
    )
    (out_ref, arrived, returned, made_back, pre, pre_in, hid, s_pre, s_pre_in, s_hid), refs = (
        refs[:10],
        refs[10:],
    )
    (gather_ref, scatter_ref), refs = refs[:2], refs[2:]
    (load_sem, fsend, frecv, rsend, rrecv, osend, orecv, xsend, xrecv, tsend, trecv), refs = (
        refs[:11],
        refs[11:],
    )
    dsend, drecv, bsend, brecv, psend, precv, hsend, hrecv, nsend, nrecv = refs

    me, col = lax.axis_index("sp"), lax.axis_index("tp")
    nz = n_sp // 2
    z, c = me // 2, lax.rem(me, 2)
    partner = z * 2 + 1 - c
    rows = pieces[0].shape[0]
    own = pl.ds(pl.multiple_of(c * rows, rows), rows)
    tall_rows = rows // LANES * LANES + (LANES if rows % LANES else 0)
    w_out_a, w_out_b, resid_ref, w_gate, w_up, w_down, sg_ref, su_ref, sd_ref = held
    experts = w_gate.shape[0]
    width = resid_ref.shape[1]
    block = arrived.shape[1]
    part = hid.shape[2] // n_tp

    def dot(a, b):
        return jnp.dot(a, b, preferred_element_type=f32)

    taken_in = [
        pltpu.make_async_copy(
            a, near[t] if t % 3 == 0 else near[t].at[own, :], load_sem.at[len(large) + t]
        )
        for t, a in enumerate(pieces)
    ]
    for copy in taken_in:
        copy.start()
    loads = [pltpu.make_async_copy(a, b, load_sem.at[i]) for i, (a, b) in enumerate(zip(large, held))]
    stops_own[...] = jnp.zeros_like(stops_own)
    heads_a, heads_b = stop_a.shape[0], stop_b.shape[0]
    stops_own[:heads_a, :rows] = stop_a[...]
    stops_own[heads_a : heads_a + heads_b, :rows] = stop_b[...]
    barrier = pltpu.get_barrier_semaphore()
    for d in range(1, n_sp):
        pl.semaphore_signal(
            barrier, inc=1, device_id={"sp": lax.rem(me + d, n_sp)}, device_id_type=MESH
        )
    for d in range(1, n_tp):
        pl.semaphore_signal(
            barrier, inc=1, device_id={"tp": lax.rem(col + d, n_tp)}, device_id_type=MESH
        )
    pl.semaphore_wait(barrier, n_sp + n_tp - 2)

    sends = []

    def remote(source, target, send, recv, where):
        copy = pltpu.make_async_remote_copy(
            src_ref=source,
            dst_ref=target,
            send_sem=send,
            recv_sem=recv,
            device_id=where,
            device_id_type=MESH,
        )
        copy.start()
        sends.append(copy)
        return copy

    def landed(ref, sem):
        pltpu.make_async_copy(ref, ref, sem).wait()

    ends = nz - 1
    names = ((6, 0), (1, 2)), ((3,), (4, 5))

    def piece(t, place):
        if t == 6:
            return stops_own
        lanes = pl.ds(pl.multiple_of(place * LANES, LANES), LANES)
        return near[t].at[:, lanes] if t % 3 == 0 else near[t].at[own, lanes]

    def spot(t, source):
        tall = stops_own.shape[0] if t == 6 else rows
        return full[t].at[pl.ds(pl.multiple_of(source * tall, tall), tall), :]

    places = [flip(z, o) for o in range(nz)]

    def push(g):
        for part_names, needed in ((names[g][1], z < ends), (names[g][0], z > 0)):

            @pl.when(needed)
            def _(part_names=part_names):
                for t in part_names:
                    for o in range(1, nz):
                        pltpu.make_async_remote_copy(
                            src_ref=piece(t, places[o]),
                            dst_ref=spot(t, me),
                            send_sem=fsend.at[o, t],
                            recv_sem=frecv.at[z, t],
                            device_id={"sp": places[o] * 2 + c},
                            device_id_type=MESH,
                        ).start()
                    pltpu.make_async_copy(piece(t, z), spot(t, me), frecv.at[z, t]).start()

    def pushed(g):
        for part_names, needed in ((names[g][1], z < ends), (names[g][0], z > 0)):

            @pl.when(needed)
            def _(part_names=part_names):
                for t in part_names:
                    for o in range(1, nz):
                        landed(piece(t, places[o]), fsend.at[o, t])

    for copy in taken_in:
        copy.wait()
    for t in (1, 2, 4, 5):
        mine = near[t].at[own, :]
        remote(mine, mine, nsend.at[t], nrecv.at[t], {"sp": partner})
    push(0)
    for load in loads:
        load.start()

    def relay(g, chip):
        for t in names[g][1]:
            mine = spot(t, chip * 2 + c)
            landed(mine, frecv.at[chip, t])
            remote(mine, mine, rsend.at[chip, t], rrecv.at[chip, t], {"sp": partner})

    def relayed(g, chip):
        for t in names[g][1]:
            landed(spot(t, chip * 2 + 1 - c), rrecv.at[chip, t])

    slot_rows = []

    def tables():
        total_experts = n_sp * experts
        kinds = lax.broadcasted_iota(jnp.int32, (total_experts, rows), 0)
        hots = [(kinds == routes_ref[t : t + 1, :]).astype(f32) for t in range(routes_ref.shape[0])]
        named = hots[0]
        for hot in hots[1:]:
            named = named + hot
        before = (
            lax.broadcasted_iota(jnp.int32, (rows, rows), 0)
            < lax.broadcasted_iota(jnp.int32, (rows, rows), 1)
        ).astype(bf16)
        earlier = dot(named.astype(bf16), before)
        aux[...] = jnp.zeros_like(aux)
        for t, hot in enumerate(hots):
            rank = jnp.sum(earlier * hot, axis=0, keepdims=True)
            slot = routes_ref[t : t + 1, :].astype(f32) * float(capacity) + rank
            slot_rows.append(slot)
            aux[t : t + 1, :rows] = slot
            aux[len(hots) + t : len(hots) + t + 1, :rows] = gates_ref[t : t + 1, :]
        spread = gather_ref.shape[0]
        tall = spread // experts

        def where_of(index, k):
            place = index + k * capacity
            for e in range(1, experts):
                place = place + jnp.where(index >= e * capacity, tall - capacity, 0)
            return place

        for k in range(2):
            index = lax.broadcasted_iota(jnp.int32, (spread, LANES), 1)
            hit = where_of(index, k) == lax.broadcasted_iota(jnp.int32, (spread, LANES), 0)
            hit = jnp.logical_and(hit, index < block)
            gather_ref[:, k * LANES : (k + 1) * LANES] = hit.astype(f32).astype(bf16)
        index = lax.broadcasted_iota(jnp.int32, (2 * block, spread), 0)
        place = jnp.where(index < block, where_of(index, 0), where_of(index - block, 1))
        hit = place == lax.broadcasted_iota(jnp.int32, (2 * block, spread), 1)
        scatter_ref[...] = hit.astype(f32).astype(bf16)

    tile = 2 * LANES

    def above(size):
        return (
            lax.broadcasted_iota(jnp.int32, (size, size), 0)
            > lax.broadcasted_iota(jnp.int32, (size, size), 1)
        ).astype(bf16)

    lane = lax.broadcasted_iota(jnp.int32, (rows, LANES), 1)
    offsets = (0, heads_a)
    fill = jnp.zeros((LANES - stops_own.shape[0], stops_own.shape[1]), f32)

    def weigh(mine, keys, stop, scale, upper, valid, carry):
        score = lax.dot_general(mine, keys, (((1,), (1,)), ((), ())), preferred_element_type=f32)
        score = score * scale + stop
        fail = jnp.log2(1.0 + jnp.exp2(jnp.minimum(score, 100.0)))
        fail = jnp.maximum(fail, score)
        hit = score - fail
        if valid is not None:
            fail = jnp.where(valid, fail, 0.0)
        after = dot(fail.astype(bf16), upper)
        weight = jnp.exp2(hit - after if carry is None else hit - after - carry)
        if valid is not None:
            weight = jnp.where(valid, weight, 0.0)
        spent = after[:, :1] + fail[:, :1]
        return weight.astype(bf16), spent if carry is None else carry + spent

    def merge(parts, size):
        merged = parts[0]
        for h in range(1, len(parts)):
            merged = jnp.where(lane // size >= h, parts[h], merged)
        return merged

    def at_home(g):
        size = groups[g][1]
        heads = LANES // size
        scale = LOG2E * size ** (-0.5)
        upper = above(2 * rows)
        valid = lax.broadcasted_iota(jnp.int32, (rows, 2 * rows), 1) < (
            lax.broadcasted_iota(jnp.int32, (rows, 2 * rows), 0) + c * rows
        )
        stop_all = jnp.concatenate([stops_own[...], fill], axis=0).T[:rows]
        for t in (3 * g + 1, 3 * g + 2):
            landed(near[t].at[pl.ds(pl.multiple_of((1 - c) * rows, rows), rows), :], nrecv.at[t])
        for u in range(groups[g][0]):
            lanes = slice(u * LANES, (u + 1) * LANES)
            query = near[3 * g][:, lanes]
            keys, values = near[3 * g + 1][:, lanes], near[3 * g + 2][:, lanes]
            parts, factors = [], []
            for h in range(heads):
                head = offsets[g] + u * heads + h
                stop = stop_all[:, head : head + 1] * LOG2E
                mine = query * ((lane // size) == h).astype(bf16) if heads > 1 else query
                weight, spent = weigh(mine, keys, stop, scale, upper, valid, None)
                parts.append(dot(weight, values))
                factors.append(jnp.exp2(-spent))
            home[2 * g][:, lanes] = merge(parts, size)
            home[2 * g + 1][:, lanes] = merge(
                [jnp.broadcast_to(f, (rows, LANES)) for f in factors], size
            )

    tables()
    at_home(0)
    push(1)
    at_home(1)
    for chip in range(ends):
        relay(0, chip)
    upper = above(tile)
    backs = []
    steps = [(g, m) for g in range(2) for m in range(1, nz)]
    for g, m in steps:
        relayed(g, m - 1)
        size = groups[g][1]
        heads = LANES // size
        q_ref, k_ref, v_ref = full[3 * g : 3 * g + 3]
        scale = LOG2E * size ** (-0.5)
        block_q = 2 * m + c
        for t in names[g][0]:
            landed(spot(t, block_q), frecv.at[m, t])
        query = q_ref[pl.ds(pl.multiple_of(block_q * rows, rows), rows), :]
        lines = stops_own.shape[0]
        stop_t = full[6][pl.ds(pl.multiple_of(block_q * lines, lines), lines), :]
        stop_all = jnp.concatenate([stop_t, fill], axis=0).T[:rows]
        reach = 2 * m * rows
        count = -(-reach // tile)
        parts = []
        for h in range(heads):
            head = offsets[g] + z * heads + h
            stop = jnp.sum(jnp.where(lane == head, stop_all, 0.0), axis=1, keepdims=True) * LOG2E
            mine = query * ((lane // size) == h).astype(bf16) if heads > 1 else query
            carry = jnp.zeros((rows, 1), f32)
            total = jnp.zeros((rows, LANES), f32)
            for i in range(count):
                if (g, m, h, i) == (0, ends, heads - 1, count // 2):
                    for chip in range(ends):
                        relay(1, chip)
                stop_at = reach - tile * i
                start = max(stop_at - tile, 0)
                wide = stop_at - start
                weight, carry = weigh(
                    mine, k_ref[start:stop_at], stop, scale, upper[:wide, :wide], None, carry
                )
                total = total + dot(weight, v_ref[start:stop_at])
            parts.append(total)
        made[g][m] = merge(parts, size).astype(bf16)
        place = attended[g].at[:, pl.ds(pl.multiple_of(z * LANES, LANES), LANES)]
        backs.append((g, m))

        @pl.when(m != z)
        def _(g=g, m=m, place=place, block_q=block_q):
            pltpu.make_async_remote_copy(
                src_ref=made[g].at[m],
                dst_ref=place,
                send_sem=osend.at[g, m],
                recv_sem=orecv.at[g, z],
                device_id={"sp": block_q},
                device_id_type=MESH,
            ).start()

        @pl.when(m == z)
        def _(g=g, m=m, place=place):
            pltpu.make_async_copy(made[g].at[m], place, orecv.at[g, z]).start()

    loads[0].wait()
    loads[1].wait()
    loads[2].wait()

    def columns(which, wide):
        return pl.ds(pl.multiple_of(which * wide, wide), wide)

    peers = [lax.rem(col + d, n_tp) for d in range(1, n_tp)] + [col]
    for g, weights in enumerate((w_out_a, w_out_b)):
        @pl.when(z == 0)
        def _(g=g):
            left_refs[g][...] = home[2 * g][...].astype(bf16)

        @pl.when(z > 0)
        def _(g=g):
            for u in range(groups[g][0]):
                lanes = slice(u * LANES, (u + 1) * LANES)
                landed(attended[g].at[:, lanes], orecv.at[g, u])
                far = home[2 * g + 1][:, lanes] * attended[g][:, lanes].astype(f32)
                left_refs[g][:, lanes] = (home[2 * g][:, lanes] + far).astype(bf16)

        left = left_refs[g][...]
        for i, peer in enumerate(peers):
            term = dot(left, weights[:, columns(peer, width)])
            if g == 0:
                partial[i] = term
                continue
            part_out[i] = (partial[i] + term).astype(bf16)
            if i < n_tp - 1:
                remote(part_out.at[i], part_in.at[i], xsend.at[i], xrecv.at[i], {"tp": peer})
    resid = resid_ref[...].astype(f32)
    mixed = part_out[n_tp - 1].astype(f32)
    for i in range(n_tp - 1):
        landed(part_in.at[i], xrecv.at[i])
        mixed = mixed + part_in[i].astype(f32)

    shaped = mixed * mix_gain[...]
    sums = jnp.zeros((rows, LANES), f32)
    for i, term in enumerate((mixed * mixed, resid * resid, resid * shaped, shaped * shaped)):
        sums = jnp.where(lane == i, jnp.sum(term, axis=1, keepdims=True), sums)
    if tall_rows > rows:
        sums = jnp.concatenate([sums, jnp.zeros((tall_rows - rows, LANES), f32)], axis=0)
    stats_out[...] = sums.T[:8]
    for d in range(1, n_tp):
        remote(
            stats_out, stats_in.at[d - 1], tsend.at[d - 1], trecv.at[d - 1], {"tp": peers[d - 1]}
        )
    sums = stats_out[...]
    for d in range(1, n_tp):
        landed(stats_in.at[d - 1], trecv.at[d - 1])
        sums = sums + stats_in[d - 1]
    sums = jnp.concatenate([sums, jnp.zeros((LANES - 8, tall_rows), f32)], axis=0).T[:rows]
    model = width * n_tp
    scale = lax.rsqrt(sums[:, 0:1] / model + epsilon)
    stream = (resid + shaped * scale).astype(bf16)
    square = sums[:, 1:2] + scale * (2.0 * sums[:, 2:3] + scale * sums[:, 3:4])
    square = jnp.maximum(square, 0.0)
    stream = stream.astype(f32)
    result_ref[...] = stream
    normed = stream * lax.rsqrt(square / model + epsilon) * ffn_gain[...]
    normed_ref[...] = normed.astype(bf16)

    chips = [flip(z, o) for o in order]
    shared = len(chips)
    seat = lax.broadcasted_iota(jnp.int32, (block, rows), 0)

    def dispatch(i):
        for k in range(2):
            peer = chips[i] * 2 + lax.rem(c + k, 2)
            seats = (seat + peer * block).astype(f32)
            chosen = seats == slot_rows[0]
            for slot in slot_rows[1:]:
                chosen = jnp.logical_or(chosen, seats == slot)
            picked = dot(chosen.astype(f32).astype(bf16), normed_ref[...]).astype(bf16)
            here = out_ref.at[2 * i + k]
            out_ref[2 * i + k] = picked
            if order[i] == 0 and k == 0:
                pltpu.make_async_copy(here, arrived.at[me], drecv.at[me]).start()
            else:
                remote(here, arrived.at[me], dsend.at[2 * i + k], drecv.at[me], {"sp": peer})

    def buffers(i):
        if i == shared:
            return s_pre, s_pre_in, s_hid
        return pre.at[i], pre_in.at[i], hid.at[i]

    def first(i):
        here, there, _ = buffers(i)
        if i == shared:
            loads[6].wait()
            loads[7].wait()
            for k, weight in enumerate((sg_ref, su_ref)):
                here[k] = dot(normed_ref[...], weight[...]).astype(bf16)
        else:
            grouped = None
            for k in range(2):
                source = chips[i] * 2 + k
                landed(arrived.at[source], drecv.at[source])
                term = dot(gather_ref[:, k * LANES : k * LANES + block], arrived[source])
                grouped = term if grouped is None else grouped + term
            grouped = grouped.astype(bf16)
            tall = grouped.shape[0] // experts
            if i == 0:
                loads[3].wait()
                loads[4].wait()
            for k, weight in enumerate((w_gate, w_up)):
                terms = [
                    dot(grouped[e * tall : (e + 1) * tall], weight[e]).astype(bf16)
                    for e in range(experts)
                ]
                spread_rows = jnp.concatenate(terms, axis=0)
                here[k] = dot(scatter_ref[...], spread_rows).astype(bf16)
        for d in range(1, n_tp):
            for k in range(2):
                remote(
                    here.at[k, :, columns(peers[d - 1], part)],
                    there.at[d - 1, k],
                    psend.at[i, d - 1, k],
                    precv.at[i, d - 1, k],
                    {"tp": peers[d - 1]},
                )

    def second(i):
        here, there, whole = buffers(i)
        sums = []
        for k in range(2):
            total = here[k, :, columns(col, part)].astype(f32)
            for d in range(1, n_tp):
                landed(there.at[d - 1, k], precv.at[i, d - 1, k])
                total = total + there[d - 1, k].astype(f32)
            sums.append(total)
        whole[:, columns(col, part)] = (sums[0] / (1.0 + jnp.exp(-sums[0])) * sums[1]).astype(bf16)
        for d in range(1, n_tp):
            mine = whole.at[:, columns(col, part)]
            remote(mine, mine, hsend.at[i, d - 1], hrecv.at[i, d - 1], {"tp": peers[d - 1]})

    kept = []

    def third(i):
        _, _, whole = buffers(i)
        for d in range(1, n_tp):
            source = lax.rem(col + n_tp - d, n_tp)
            landed(whole.at[:, columns(source, part)], hrecv.at[i, d - 1])
        if i == shared:
            loads[8].wait()
            result_ref[...] = result_ref[...] + dot(whole[...], sd_ref[...])
            return
        hidden = whole[...]
        grouped = dot(gather_ref[:, :block], hidden[:block]) + dot(
            gather_ref[:, LANES : LANES + block], hidden[block:]
        )
        grouped = grouped.astype(bf16)
        tall = grouped.shape[0] // experts
        if i == 0:
            loads[5].wait()
        terms = [
            dot(grouped[e * tall : (e + 1) * tall], w_down[e]).astype(bf16) for e in range(experts)
        ]
        terms = dot(scatter_ref[...], jnp.concatenate(terms, axis=0))
        for k in range(2):
            source = chips[i] * 2 + k
            made_back[i, k] = terms[k * block : (k + 1) * block].astype(bf16)
            if order[i] == 0:

                @pl.when(source != me)
                def _():
                    pltpu.make_async_remote_copy(
                        src_ref=made_back.at[i, k],
                        dst_ref=returned.at[me],
                        send_sem=bsend.at[i, k],
                        recv_sem=brecv.at[me],
                        device_id={"sp": source},
                        device_id_type=MESH,
                    ).start()

                @pl.when(source == me)
                def _():
                    pltpu.make_async_copy(made_back.at[i, k], returned.at[me], brecv.at[me]).start()

                kept.append((i, k, source))
            else:
                remote(
                    made_back.at[i, k],
                    returned.at[me],
                    bsend.at[i, k],
                    brecv.at[me],
                    {"sp": source},
                )

    top_count = routes_ref.shape[0]
    turned = aux[...].T[:rows]
    taken = lax.broadcasted_iota(jnp.int32, (rows, block), 1)

    def combine(i):
        total = result_ref[...]
        for k in range(2):
            source = chips[i] * 2 + k
            landed(returned.at[source], brecv.at[source])
            seats = (taken + source * block).astype(f32)
            gated = jnp.zeros(seats.shape, f32)
            for t in range(top_count):
                gate = turned[:, top_count + t : top_count + t + 1]
                gated = gated + jnp.where(seats == turned[:, t : t + 1], gate, 0.0)
            high = gated.astype(bf16)
            low = (gated - high.astype(f32)).astype(bf16)
            total = total + dot(high, returned[source]) + dot(low, returned[source])
        result_ref[...] = total

    dispatch(1)
    dispatch(0)
    first(shared)
    first(0)
    dispatch(2)
    dispatch(3)
    first(1)
    second(0)
    first(2)
    second(1)
    first(3)
    third(0)
    second(2)
    third(1)
    second(3)
    third(2)
    second(shared)
    third(3)
    combine(0)
    combine(1)
    third(shared)
    combine(2)
    combine(3)
    for copy in sends:
        copy.wait_send()
    pushed(0)
    pushed(1)
    for g, m in backs:

        @pl.when(m != z)
        def _(g=g, m=m):
            landed(made[g].at[m], osend.at[g, m])

    for i, k, source in kept:

        @pl.when(source != me)
        def _(i=i, k=k):
            landed(made_back.at[i, k], bsend.at[i, k])


def layer(n_sp, n_tp, groups, capacity, arrays, small, large):
    f32, bf16 = jnp.float32, jnp.bfloat16
    rows = arrays[0].shape[0]
    resid, w_gate = large[2], large[3]
    width = resid.shape[1]
    experts, hidden_width = w_gate.shape[0], w_gate.shape[2]
    block = experts * capacity
    nz = n_sp // 2
    order = (0,) + tuple(range(nz // 2, nz)) + tuple(range(nz // 2 - 1, 0, -1))
    wide = -(-rows // LANES) * LANES
    lines = -(-(small[0].shape[0] + small[1].shape[0]) // 8) * 8
    tall = -(-2 * capacity // 16) * 16
    part = hidden_width // n_tp
    dma = pltpu.SemaphoreType.DMA
    vmem = pltpu.VMEM
    anywhere = pl.BlockSpec(memory_space=pl.ANY)
    scratch = (
        [vmem((n_sp * rows, LANES), bf16)] * 6
        + [vmem((n_sp * lines, wide), f32)]
        + [vmem(((1 if t % 3 == 0 else 2) * rows, a.shape[1]), bf16) for t, a in enumerate(arrays)]
        + [vmem((rows, units * LANES), f32) for units, _ in groups for _ in range(2)]
        + [vmem((rows, units * LANES), bf16) for units, _ in groups]
        + [vmem((nz, rows, LANES), bf16)] * 2
        + [vmem((rows, units * LANES), bf16) for units, _ in groups]
        + [vmem(a.shape, a.dtype) for a in large]
        + [
            vmem((lines, wide), f32),
            vmem((n_tp, rows, width), f32),
            vmem((n_tp, rows, width), bf16),
            vmem((n_tp - 1, rows, width), bf16),
            vmem((LANES, wide), f32),
            vmem((8, wide), f32),
            vmem((n_tp - 1, 8, wide), f32),
            vmem((rows, width), bf16),
        ]
        + [
            vmem((n_sp, block, width), bf16),
            vmem((n_sp, block, width), bf16),
            vmem((n_sp, block, width), bf16),
            vmem((nz, 2, block, width), bf16),
            vmem((nz, 2, 2 * block, hidden_width), bf16),
            vmem((nz, n_tp - 1, 2, 2 * block, part), bf16),
            vmem((nz, 2 * block, hidden_width), bf16),
            vmem((2, rows, hidden_width), bf16),
            vmem((n_tp - 1, 2, rows, part), bf16),
            vmem((rows, hidden_width), bf16),
        ]
        + [vmem((experts * tall, 2 * LANES), bf16), vmem((2 * block, experts * tall), bf16)]
        + [dma((len(large) + len(arrays),))]
        + [dma((nz, 7))] * 4
        + [dma((2, nz))] * 2
        + [dma((n_tp - 1,))] * 4
        + [dma((n_sp,)), dma((n_sp,)), dma((nz, 2)), dma((n_sp,))]
        + [dma((nz + 1, n_tp - 1, 2))] * 2
        + [dma((nz + 1, n_tp - 1))] * 2
        + [dma((6,))] * 2
    )
    return pl.pallas_call(
        functools.partial(layer_kernel, n_sp, n_tp, groups, capacity, order),
        out_shape=pltpu.VMEM((rows, width), f32),
        in_specs=[anywhere] * 6 + [VM] * 6 + [anywhere] * 9,
        out_specs=VM,
        scratch_shapes=scratch,
        compiler_params=params(9),
        name="layer",
    )(*arrays, *small, *large)


def shards(
    n_sp,
    n_tp,
    query_a,
    key_a,
    value_a,
    query_b,
    key_b,
    value_b,
    stop_a,
    stop_b,
    out_a,
    out_b,
    resid,
    mix_gain,
    ffn_gain,
    routes,
    gates,
    exp_gate,
    exp_up,
    exp_down,
    sh_gate,
    sh_up,
    sh_down,
):
    f32, bf16 = jnp.float32, jnp.bfloat16
    rows = query_a.shape[0]
    heads_a, heads_b = stop_a.shape[1], stop_b.shape[1]
    units_a, units_b = query_a.shape[1] // LANES, query_b.shape[1] // LANES
    width = resid.shape[1]
    model = width * n_tp

    local_experts = exp_gate.shape[0]
    experts = local_experts * n_sp
    top_count = routes.shape[1]
    capacity = max(1, (3 * rows * top_count + 2 * experts - 1) // (2 * experts))
    block = local_experts * capacity
    hidden_width = exp_gate.shape[2]
    groups = ((units_a, query_a.shape[1] // heads_a), (units_b, query_b.shape[1] // heads_b))
    fused = (
        (hidden_width // n_tp) % LANES == 0
        and width % LANES == 0
        and block % 8 == 0
        and block <= LANES
        and exp_gate.shape == exp_down.shape
        and all(2 * units == n_sp for units, _ in groups)
        and (n_sp // 2) & (n_sp // 2 - 1) == 0
        and 2 * rows <= 4 * LANES
        and 2 * rows % LANES == 0
        and rows % 16 == 0
    )
    if fused:
        arrays = (query_a, key_a, value_a, query_b, key_b, value_b)
        small = (stop_a.T, stop_b.T, routes.T, gates.T, mix_gain[None, :], ffn_gain[None, :])
        large = (out_a, out_b, resid, exp_gate, exp_up, exp_down, sh_gate, sh_up, sh_down)
        return layer(n_sp, n_tp, groups, capacity, arrays, small, large).astype(bf16)

    flat_routes = routes.reshape(-1)
    onehot = (flat_routes[:, None] == jnp.arange(experts, dtype=jnp.int32)[None, :]).astype(f32)
    pairs = rows * top_count
    before = (jnp.arange(pairs)[:, None] > jnp.arange(pairs)[None, :]).astype(bf16)
    earlier = jnp.dot(before, onehot.astype(bf16), preferred_element_type=f32)
    slot = flat_routes * capacity + jnp.sum(earlier * onehot, axis=1).astype(jnp.int32)
    slot = slot.reshape(rows, top_count)
    slots = jnp.arange(experts * capacity, dtype=jnp.int32)
    chosen = slot[:, :, None] == slots[None, None, :]
    chooser = jnp.sum(chosen.astype(f32), axis=1).astype(bf16)
    gated = jnp.sum(jnp.where(chosen, gates[:, :, None], 0.0), axis=1)
    gated_high = gated.astype(bf16)
    gated_low = (gated - gated_high.astype(f32)).astype(bf16)

    stops = jnp.concatenate([stop_a, stop_b], axis=1)
    lines = -(-stops.shape[1] // 8) * 8
    wide = -(-rows // LANES) * LANES
    stops = jnp.pad(stops.T, ((0, lines - stops.shape[1]), (0, wide - rows)))
    arrays = (query_a, key_a, value_a, query_b, key_b, value_b, stops)
    attended_a, attended_b = stick(n_sp, rows, arrays, groups, (0, heads_a), 0)

    partial_value = jnp.dot(attended_a, out_a, preferred_element_type=f32)
    partial_value = partial_value + jnp.dot(attended_b, out_b, preferred_element_type=f32)
    (pieces,) = exchange("tp", n_tp, (partial_value.astype(bf16),), ("cols",), 2)
    mixed = jnp.sum(pieces.astype(f32), axis=0)
    resid_f = resid.astype(f32)
    shaped = mixed * mix_gain[None, :]
    sums = jnp.stack(
        [
            jnp.sum(mixed * mixed, axis=1),
            jnp.sum(resid_f * resid_f, axis=1),
            jnp.sum(resid_f * shaped, axis=1),
            jnp.sum(shaped * shaped, axis=1),
        ]
    )
    sums = jnp.pad(sums, ((0, 4), (0, wide - rows)))
    (sums,) = exchange("tp", n_tp, (sums,), ("all",), 3)
    sums = jnp.sum(sums, axis=0)[:4, :rows]
    scale = lax.rsqrt(sums[0] / model + epsilon)
    stream = (resid_f + shaped * scale[:, None]).astype(bf16)
    square = jnp.maximum(sums[1] + scale * (2.0 * sums[2] + scale * sums[3]), 0.0)
    stream_f = stream.astype(f32)
    normed = (stream_f * lax.rsqrt(square / model + epsilon)[:, None] * ffn_gain[None, :]).astype(bf16)

    outgoing = lax.dot_general(chooser, normed, (((0,), (0,)), ((), ())), preferred_element_type=f32)
    outgoing = outgoing.astype(bf16).reshape(n_sp, local_experts * capacity, width)
    (arrived,) = exchange("sp", n_sp, (outgoing,), ("lead",), 4)
    arrived = arrived.reshape(n_sp, local_experts, capacity, width)
    arrived = jnp.transpose(arrived, (1, 0, 2, 3)).reshape(local_experts, n_sp * capacity, width)

    shared_parts = [
        jnp.dot(normed, w, preferred_element_type=f32).astype(bf16) for w in (sh_gate, sh_up)
    ]
    expert_parts = [
        jnp.einsum("erd,edf->erf", arrived, w, preferred_element_type=f32)
        .astype(bf16)
        .reshape(local_experts * n_sp * capacity, -1)
        for w in (exp_gate, exp_up)
    ]
    parts = exchange("tp", n_tp, (*expert_parts, *shared_parts), ("cols",) * 4, 5)
    gate_pre, up_pre, shared_gate, shared_up = [jnp.sum(p.astype(f32), axis=0) for p in parts]
    hidden = (jax.nn.silu(gate_pre) * up_pre).astype(bf16)
    shared_hidden = (jax.nn.silu(shared_gate) * shared_up).astype(bf16)
    hidden, shared_hidden = exchange("tp", n_tp, (hidden, shared_hidden), ("side",) * 2, 6)

    shared_out = jnp.dot(shared_hidden, sh_down, preferred_element_type=f32)
    hidden = hidden.reshape(local_experts, n_sp * capacity, -1)
    produced = jnp.einsum("erf,efd->erd", hidden, exp_down, preferred_element_type=f32).astype(bf16)
    produced = produced.reshape(local_experts, n_sp, capacity, width)
    produced = jnp.transpose(produced, (1, 0, 2, 3)).reshape(n_sp, local_experts * capacity, width)
    (returned,) = exchange("sp", n_sp, (produced,), ("lead",), 7)
    flat_back = returned.reshape(experts * capacity, width)
    routed = jnp.dot(gated_high, flat_back, preferred_element_type=f32)
    routed = routed + jnp.dot(gated_low, flat_back, preferred_element_type=f32)
    moe = routed + shared_out
    return (stream_f + moe).astype(bf16)


def solution(mesh):
    return jax.shard_map(
        functools.partial(shards, mesh.shape["sp"], mesh.shape["tp"]),
        mesh=mesh,
        in_specs=(
            P("sp", "tp"),
            P("sp", "tp"),
            P("sp", "tp"),
            P("sp", "tp"),
            P("sp", "tp"),
            P("sp", "tp"),
            P("sp", "tp"),
            P("sp", "tp"),
            P("tp", None),
            P("tp", None),
            P("sp", "tp"),
            P("tp"),
            P("tp"),
            P("sp", None),
            P("sp", None),
            P("sp", "tp", None),
            P("sp", "tp", None),
            P("sp", None, "tp"),
            P("tp", None),
            P("tp", None),
            P(None, "tp"),
        ),
        out_specs=P("sp", "tp"),
        check_vma=False,
    )
```
